32 devices in a mesh: fs: 8 (over z, x), tp: 4 (over y, core).
Axes of the slice: x: 2, y: 2, z: 4, core: 2. Of those that a mesh axis runs over, the one named last changes fastest.
Arguments:
- tokens: bfloat16 [8192, 2048], P(('fs', 'tp')), may hold values from -6 to 6
- gate_pre: bfloat16 [8192, 5632], P('fs', 'tp'), may hold values from -6 to 6
- value_pre: bfloat16 [8192, 5632], P('fs', 'tp'), may hold values from -6 to 6
- up_gate_w: bfloat16 [2048, 5632], P('fs', 'tp'), may hold values from -0.078125 to 0.078125
- up_value_w: bfloat16 [2048, 5632], P('fs', 'tp'), may hold values from -0.078125 to 0.078125
- conv_weight: float32 [3, 5632], P(None, 'tp'), may hold values from -3 to 3
- conv_bias: float32 [5632], P('tp'), may hold values from -3 to 3
- hidden_grad: bfloat16 [8192, 5632], P('fs', 'tp'), may hold values from -6 to 6
Outputs:
- input_grad: bfloat16 [8192, 2048], P(('fs', 'tp'))
- up_gate_grad: float32 [2048, 5632], P('fs', 'tp')
- up_value_grad: float32 [2048, 5632], P('fs', 'tp')
- conv_weight_grad: float32 [3, 5632], P(None, 'tp')
- conv_bias_grad: float32 [5632], P('tp')
The draws below stay inside these ranges and needn't reach their ends.
All inputs are finite; a program needn't handle non-finite values.
Results may differ from the reference program's by a relative error of at most 0.013.
Values may be sent and summed in bfloat16 or wider, within the bound.
A program may use at most 128 MiB of HBM per device.

```python
import jax
import jax.numpy as jnp
from jax import lax

D = 2048
FF = 5632
ROWS = 1024
TOKENS = 8192
N_FS = 8
N_TP = 4


def with_spikes(result, rng, source, target, shards_of, factor):
    owner, partner = [(jnp.arange(result.shape[dim]) // (result.shape[dim] // shards_of)).reshape([-1 if axis == dim else 1 for axis in range(result.ndim)]) for dim in (source, target)]
    chosen = jax.random.permutation(rng, shards_of)[partner]
    strong = (owner == chosen) | (owner == (partner + shards_of // 2) % shards_of)
    return jnp.where(strong, factor * result, result)


def block_scale(stream_key, shape, cuts, low, largest):
    def one(dim, blocks):
        draws = jax.random.uniform(jax.random.fold_in(jax.random.fold_in(stream_key, 6), dim), (blocks,), jnp.float32, low / len(cuts), largest / len(cuts))
        return jnp.repeat(jnp.exp(draws), shape[dim] // blocks).reshape((-1,) + (1,) * (len(shape) - dim - 1))

    loudness = one(*cuts[0])
    for cut in cuts[1:]:
        loudness = loudness * one(*cut)
    return loudness


def scatter_about(stream_key, dims, spread, limit, shards=(), kind=jnp.bfloat16):
    entries = spread * jax.random.normal(stream_key, dims, jnp.float32)
    if shards:
        entries = entries * block_scale(stream_key, dims, shards, -0.22, 0.18)
    return jnp.clip(entries, -limit, limit).astype(kind)


def heavy_noise(stream_key, dims, deviation, reach, shards, heavy, dtype=jnp.bfloat16):
    result = deviation * jax.random.normal(stream_key, dims, jnp.float32)
    if shards:
        result = result * block_scale(stream_key, dims, shards, -0.22, 0.18)
    return jnp.clip(with_spikes(result, jax.random.fold_in(stream_key, 3), *heavy), -reach, reach).astype(dtype)


def setup_inputs(seed: int = 0) -> dict:
    splits = jax.random.split(jax.random.key(seed), 9)
    tokens = scatter_about(splits[0], (TOKENS, D), 1.0, 6.0, ((0, 32),))
    gate_pre = scatter_about(splits[1], (TOKENS, FF), 1.0, 6.0, ((0, 8), (1, 4)))
    value_pre = scatter_about(splits[2], (TOKENS, FF), 1.0, 6.0, ((0, 8), (1, 4)))
    up_gate_w = scatter_about(splits[3], (D, FF), FF ** -0.5, 0.078125, ((0, 8), (1, 4)))
    up_value_w = scatter_about(splits[4], (D, FF), FF ** -0.5, 0.078125, ((0, 8), (1, 4)))
    conv_weight = scatter_about(splits[5], (3, FF), 0.6, 3.0, ((1, 4),), jnp.float32)
    conv_bias = scatter_about(splits[6], (FF,), 0.5, 3.0, ((0, 4),), jnp.float32)
    hidden_grad = heavy_noise(splits[7], (TOKENS, FF), 1.0, 6.0, ((0, 8), (1, 4)), (0, 1, 8, 2.0))
    return dict(tokens=tokens, gate_pre=gate_pre, value_pre=value_pre, up_gate_w=up_gate_w, up_value_w=up_value_w, conv_weight=conv_weight, conv_bias=conv_bias, hidden_grad=hidden_grad)


def conv_forward(pre_gate, conv_weight, conv_bias):
    length = pre_gate.shape[0]
    padded = jnp.pad(pre_gate, ((2, 0), (0, 0)))
    return conv_bias + conv_weight[0] * padded[:length] + conv_weight[1] * padded[1:length + 1] + conv_weight[2] * padded[2:]

def reference(tokens, gate_pre, value_pre, up_gate_w, up_value_w, conv_weight, conv_bias, hidden_grad):
    col_count = FF // N_TP
    scale = float(TOKENS) ** (-0.5)

    def one_seq(carry, items):
        tok_rows, gate_rows, value_rows, grad_rows = items
        gate_float = gate_rows.astype(jnp.float32)
        gate_conv = conv_forward(gate_float, conv_weight, conv_bias)
        active, gelu_back = jax.vjp(jax.nn.gelu, gate_conv)
        grad_float = grad_rows.astype(jnp.float32)
        value_grad = (grad_float * active).astype(jnp.bfloat16)
        conv_grad = gelu_back(grad_float * value_rows.astype(jnp.float32))[0]
        shifted = jnp.pad(conv_grad, ((0, 2), (0, 0)))
        gate_grad = (conv_weight[2] * conv_grad + conv_weight[1] * shifted[1:ROWS + 1] + conv_weight[0] * shifted[2:]).astype(jnp.bfloat16)
        padded = jnp.pad(gate_float, ((2, 0), (0, 0)))
        conv_terms = jnp.stack([lax.optimization_barrier(jnp.sum(conv_grad * padded[:ROWS], axis=0)), lax.optimization_barrier(jnp.sum(conv_grad * padded[1:ROWS + 1], axis=0)), lax.optimization_barrier(jnp.sum(conv_grad * padded[2:], axis=0)), lax.optimization_barrier(jnp.sum(conv_grad, axis=0))])
        gate_term = jnp.dot(tok_rows.T, gate_grad, preferred_element_type=jnp.float32)
        value_term = jnp.dot(tok_rows.T, value_grad, preferred_element_type=jnp.float32)
        parts = jnp.einsum('rkc,dkc->krd', gate_grad.reshape(ROWS, N_TP, col_count).astype(jnp.float32), up_gate_w.reshape(D, N_TP, col_count).astype(jnp.float32))
        parts = parts + jnp.einsum('rkc,dkc->krd', value_grad.reshape(ROWS, N_TP, col_count).astype(jnp.float32), up_value_w.reshape(D, N_TP, col_count).astype(jnp.float32))
        rounded = lax.optimization_barrier(parts.astype(jnp.bfloat16))
        input_rows = lax.optimization_barrier(jnp.sum(rounded.astype(jnp.float32), axis=0)).astype(jnp.bfloat16)
        return ((carry[0] + gate_term, carry[1] + value_term, carry[2] + conv_terms), input_rows)
    init = (jnp.zeros((D, FF), jnp.float32), jnp.zeros((D, FF), jnp.float32), jnp.zeros((4, FF), jnp.float32))
    items = (tokens.reshape(N_FS, ROWS, D), gate_pre.reshape(N_FS, ROWS, FF), value_pre.reshape(N_FS, ROWS, FF), hidden_grad.reshape(N_FS, ROWS, FF))
    totals, input_seqs = lax.scan(one_seq, init, items)
    input_grad = input_seqs.reshape(TOKENS, D)
    conv_total = totals[2] * scale
    return (input_grad, totals[0] * scale, totals[1] * scale, conv_total[:3], conv_total[3])
```

```python
import functools
import math

import jax
import jax.numpy as jnp
from jax import lax
from jax.experimental import pallas as pl
from jax.experimental.pallas import tpu as pltpu
from jax.sharding import PartitionSpec as P

MESH = pl.DeviceIdType.MESH
F32, BF16 = jnp.float32, jnp.bfloat16
PAD = 16
LANES = 128


def dot_rows(left, right):
    return lax.dot_general(left, right, (((1,), (0,)), ((), ())), preferred_element_type=F32)


def dot_cols(left, right):
    return lax.dot_general(left, right, (((1,), (1,)), ((), ())), preferred_element_type=F32)


def tiles(width, tile, body):
    whole = width // tile

    @pl.loop(0, whole)
    def _(n):
        body(pl.multiple_of(n * tile, tile), tile)

    if width % tile:
        body(whole * tile, width % tile)


def kernel(
    line, n_tp, scale,
    tok_hbm, gate_hbm, value_hbm, wg_hbm, wv_hbm, hid_hbm, taps, bias,
    ig_out, gate_out, value_out, conv_out,
    wg, wv, tok, tok_t, gst, hst, vst, cgs, acc, vfin, gfin,
    sb, sa, pair_in, vx_out, vx_in, ig_send, ig_recv, ig_sum, conv_recv, csum,
    load_sem, tok_ss, tok_rs,
    gu, gd, gx, rg, vu, vd, vx, rv,
    bu, bd, bru, brd, au, ad, aru, ard, qs, qr, xs, xr, ig_ss, ig_rs, cs, cr,
):
    me, tp = lax.axis_index("fs"), lax.axis_index("tp")
    i, j = me // 2, me % 2
    other = 2 * i + 1 - j
    up, down = me + 2, me - 2
    has_up, has_down = i < line - 1, i > 0
    n_fs = 2 * line
    rows = hid_hbm.shape[0]
    cols = hid_hbm.shape[1]
    shard = wg_hbm.shape[0]
    own_tok = tok_hbm.shape[0]
    width = tok_hbm.shape[1]
    rounds = n_fs.bit_length() - 1

    def remote(src, dst, ss, rs, fs=None, to_tp=None):
        where = {"fs": me if fs is None else fs, "tp": tp if to_tp is None else to_tp}
        return pltpu.make_async_remote_copy(
            src_ref=src, dst_ref=dst, send_sem=ss, recv_sem=rs, device_id=where, device_id_type=MESH
        )

    def gate_up(o, src):
        return remote(src, wg.at[o], gu.at[o // 2], rg.at[o], up)

    def gate_down(o, src):
        return remote(src, wg.at[o], gd.at[o // 2], rg.at[o], down)

    def gate_pair(o, src):
        return remote(src, wg.at[o], gx.at[o // 2], rg.at[o], other)

    def value_up(o, src):
        return remote(src, wv.at[o], vu.at[o], rv.at[o], up)

    def value_down(o, src):
        return remote(src, wv.at[o], vd.at[o], rv.at[o], down)

    def value_pair(src):
        return remote(src, wv.at[me], vx, rv.at[me], other)

    loads = [
        pltpu.make_async_copy(tok_hbm, tok, load_sem.at[0]),
        pltpu.make_async_copy(gate_hbm, gst.at[pl.ds(PAD, rows)], load_sem.at[1]),
        pltpu.make_async_copy(hid_hbm, hst, load_sem.at[2]),
        pltpu.make_async_copy(value_hbm, vst.at[pl.ds(0, rows)], load_sem.at[3]),
        pltpu.make_async_copy(wg_hbm, wg.at[me], load_sem.at[4]),
        pltpu.make_async_copy(wv_hbm, wv.at[me], load_sem.at[5]),
    ]
    value_pair(wv_hbm).start()
    gate_pair(me, wg_hbm).start()

    @pl.when(has_up)
    def _():
        gate_up(me, wg_hbm).start()
        value_up(me, wv_hbm).start()

    @pl.when(has_down)
    def _():
        gate_down(me, wg_hbm).start()
        value_down(me, wv_hbm).start()

    for load in loads:
        load.start()

    loads[0].wait()
    turn = 256

    @pl.loop(0, width // turn)
    def _(n):
        at = pl.multiple_of(n * turn, turn)
        tok_t[pl.ds(at, turn), pl.ds(pl.multiple_of(tp * own_tok, own_tok), own_tok)] = tok[
            :, pl.ds(at, turn)
        ].T

    def tok_piece(d, source):
        return tok_t.at[
            pl.ds(pl.multiple_of(d * 2 * shard, 2 * shard), 2 * shard),
            pl.ds(pl.multiple_of(source * own_tok, own_tok), own_tok),
        ]

    def far(n):
        return jnp.where(n % 2 == 0, line - 1 - n // 2, n // 2)

    def tok_copy(d, step):
        peer = (tp + step) % n_tp
        return remote(tok_piece(d, tp), tok_piece(d, tp), tok_ss.at[step, d], tok_rs.at[tp, d], to_tp=peer)

    def tok_landed(d):
        @pl.loop(1, n_tp)
        def _(step):
            source = (tp + step) % n_tp
            remote(tok_piece(d, source), tok_piece(d, source), tok_ss.at[0, d], tok_rs.at[source, d]).wait_recv()

    @pl.loop(0, line)
    def _(n):
        @pl.loop(1, n_tp)
        def _(step):
            tok_copy(far(n), step).start()

    loads[1].wait()
    loads[2].wait()
    loads[3].wait()
    chunk = 64
    root = math.sqrt(2.0 / math.pi)

    def elementwise(at, size):
        cut = pl.ds(at, size)
        gst[pl.ds(0, PAD), cut] = jnp.zeros((PAD, size), BF16)
        w0, w1, w2 = (taps[pl.ds(k, 1), cut] for k in range(3))
        b = bias[:, cut]

        def forward(n, sums):
            r = pl.multiple_of(n * chunk, chunk)
            wide = gst[pl.ds(r, PAD + chunk), cut].astype(F32)
            x0 = wide[PAD:]
            x1 = pltpu.roll(wide, 1, 0)[PAD:]
            x2 = pltpu.roll(wide, 2, 0)[PAD:]
            z = b + w0 * x2 + w1 * x1 + w2 * x0
            sq = z * z
            th = jnp.tanh(root * (z + 0.044715 * (sq * z)))
            cdf = 0.5 * (1.0 + th)
            h = hst[pl.ds(r, chunk), cut].astype(F32)
            v = vst[pl.ds(r, chunk), cut].astype(F32)
            hst[pl.ds(r, chunk), cut] = (h * (z * cdf)).astype(BF16)
            slope = cdf + (0.5 * z) * (1.0 - th * th) * (root + (3.0 * 0.044715 * root) * sq)
            cg = slope * (h * v)
            cgs[pl.ds(r, chunk), pl.ds(0, size)] = cg

            def fold(term):
                return jnp.sum(term.reshape(chunk // 8, 8, size), axis=0)

            return tuple(s + fold(t) for s, t in zip(sums, (cg * x2, cg * x1, cg * x0, cg)))

        zero = jnp.zeros((8, size), F32)
        sums = lax.fori_loop(0, rows // chunk, forward, (zero,) * 4)
        for k in range(4):
            csum[pl.ds(k, 1), cut] = jnp.sum(sums[k], axis=0, keepdims=True)
        cgs[pl.ds(rows, 8), pl.ds(0, size)] = jnp.zeros((8, size), F32)

        @pl.loop(0, rows // chunk)
        def _(n):
            r = pl.multiple_of(n * chunk, chunk)
            wide = cgs[pl.ds(r, chunk + 8), pl.ds(0, size)]
            g1 = pltpu.roll(wide, chunk + 7, 0)[:chunk]
            g2 = pltpu.roll(wide, chunk + 6, 0)[:chunk]
            gst[pl.ds(PAD + r, chunk), cut] = (w2 * wide[:chunk] + w1 * g1 + w0 * g2).astype(BF16)

    tiles(cols, LANES, elementwise)

    def conv_copy(r):
        return remote(csum.at[pl.ds(0, 4)], conv_recv.at[r], cs.at[r], cr.at[r], me ^ (1 << r))

    def conv_add(r):
        conv_copy(r).wait_send()
        conv_copy(r).wait_recv()
        csum[pl.ds(0, 4), :] += conv_recv[r]

    conv_copy(0).start()

    remote(wv.at[other], wv.at[other], vx, rv.at[other]).wait_recv()

    @pl.when(has_up)
    def _():
        value_up(other, wv.at[other]).start()

    @pl.when(has_down)
    def _():
        value_down(other, wv.at[other]).start()

    def gather(t):
        low, high = i - t - 1, i + t + 1

        @pl.when(low >= 0)
        def _():
            o = 2 * low + j
            gate_up(o, wg.at[o]).wait_recv()

            @pl.when(has_up)
            def _():
                gate_up(o, wg.at[o]).start()

            gate_pair(o, wg.at[o]).start()

        @pl.when(high < line)
        def _():
            o = 2 * high + j
            gate_down(o, wg.at[o]).wait_recv()

            @pl.when(has_down)
            def _():
                gate_down(o, wg.at[o]).start()

            gate_pair(o, wg.at[o]).start()

        for flip in range(2):
            jd = j if flip == 0 else 1 - j

            @pl.when(low >= 0)
            def _():
                o = 2 * low + jd
                value_up(o, wv.at[o]).wait_recv()

                @pl.when(has_up)
                def _():
                    value_up(o, wv.at[o]).start()

            @pl.when(high < line)
            def _():
                o = 2 * high + jd
                value_down(o, wv.at[o]).wait_recv()

                @pl.when(has_down)
                def _():
                    value_down(o, wv.at[o]).start()

    def gate_grad(cut):
        return gst[pl.ds(PAD, rows), cut]

    def value_grad(cut):
        return hst[:, cut]

    def term(grad, o):
        left = pl.ds(pl.multiple_of(o * shard, shard), shard)

        def one(at, size):
            cut = pl.ds(at, size)
            acc[:, cut] = dot_rows(tok_t[left, :], grad(cut))

        tiles(cols, 256, one)

    step_rows = 16

    def each_rows(body):
        @pl.loop(0, shard // step_rows)
        def _(n):
            body(pl.ds(pl.multiple_of(n * step_rows, step_rows), step_rows))

    def put(dst, *more):
        def body(cut):
            total = acc[cut, :]
            for ref in more:
                total = total + ref[cut, :].astype(F32)
            dst[cut, :] = total.astype(dst.dtype)

        each_rows(body)

    def landing(d, receiver):
        return jnp.where(d == receiver, line, d)

    def hop(grad, slots, o, d, going_up, ss, rs, extra=None):
        term(grad, o)
        more = () if extra is None else (extra(),)
        slot = slots.at[d]
        came = has_down if going_up else has_up
        if going_up:
            arrived = remote(slot, slot, ss, rs)
            sent = remote(slot, slot, ss, rs, up)
        else:
            arrived = remote(slot, slot, ss, rs)
            sent = remote(slot, slots.at[landing(d, i - 1)], ss, rs, down)

        @pl.when(came)
        def _():
            arrived.wait_recv()
            put(slot, slot, *more)

        @pl.when(jnp.logical_not(came))
        def _():
            put(slot, *more)

        sent.start()

    def up_row(tt):
        return line - 1 - tt + i

    def down_row(tt):
        return tt - line + 1 + i

    def value_step(tt):
        for jd in range(2):
            @pl.when(tt >= i)
            def _():
                d = up_row(tt)
                hop(value_grad, sb.at[jd], 2 * d + jd, d, True, bu.at[jd, d], bru.at[jd, d])

            @pl.when(tt >= line - 1 - i)
            def _():
                d = down_row(tt)
                hop(value_grad, sb.at[jd], 2 * d + jd, d, False, bd.at[jd, d], brd.at[jd, d])

    def pair_copy(d):
        return remote(vst.at[pl.ds(pl.multiple_of(d * shard, shard), shard)], pair_in.at[d], qs.at[d], qr.at[d], other)

    def pair_term(n):
        d = far(n)
        term(gate_grad, 2 * d + 1 - j)
        put(vst.at[pl.ds(pl.multiple_of(d * shard, shard), shard)])
        pair_copy(d).start()

    def from_pair(d):
        def get():
            pair_copy(d).wait_recv()
            return pair_in.at[d]

        return get

    def gate_step(tt):
        @pl.when(tt >= i)
        def _():
            d = up_row(tt)
            hop(gate_grad, sa, 2 * d + j, d, True, au.at[d], aru.at[d], from_pair(d))

        @pl.when(tt >= line - 1 - i)
        def _():
            d = down_row(tt)
            hop(gate_grad, sa, 2 * d + j, d, False, ad.at[d], ard.at[d], from_pair(d))

    def share_copy(k, o):
        return remote(ig_send.at[k, o], ig_recv.at[tp, o], ig_ss.at[k, o], ig_rs.at[tp, o], to_tp=k)

    def share(o):
        @pl.loop(0, n_tp)
        def _(k):
            at = pl.multiple_of(k * own_tok, own_tok)
            part = dot_cols(gst[pl.ds(PAD + at, own_tok), :], wg[o]) + dot_cols(hst[pl.ds(at, own_tok), :], wv[o])
            ig_send[k, o] = part.astype(BF16)

            @pl.when(k != tp)
            def _():
                share_copy(k, o).start()

    def share_line(t):
        for at in (i - t, i + t):
            @pl.when((at >= 0) & (at < line))
            def _():
                share(2 * at + j)

    def share_pair(t, both=True):
        for at in (i - t, i + t)[: 2 if both else 1]:
            @pl.when((at >= 0) & (at < line))
            def _():
                o = 2 * at + 1 - j
                gate_pair(o, wg.at[o]).wait_recv()
                share(o)

    loads[4].wait()
    loads[5].wait()

    @pl.loop(0, line)
    def _(n):
        tok_landed(far(n))

    pair_term(0)
    value_step(0)
    share(me)

    @pl.loop(1, line - 1)
    def _(tt):
        gather(tt - 1)
        pair_term(tt)

        @pl.when(tt < rounds)
        def _():
            conv_add(tt - 1)
            conv_copy(tt).start()

        value_step(tt)
        share_line(tt)

        @pl.when(tt == 1)
        def _():
            share_pair(0, False)

        @pl.when(tt > 1)
        def _():
            share_pair(tt - 1)

    gather(line - 2)
    pair_term(line - 1)
    conv_add(rounds - 1)
    share_line(line - 1)

    gate_step(0)
    share_pair(line - 2)

    @pl.loop(1, line - 1)
    def _(tt):
        gate_step(tt)

    def arrive(slots, ru, rd):
        @pl.when(has_down)
        def _():
            remote(slots.at[i], slots.at[i], xs, ru.at[i]).wait_recv()
            put(acc, slots.at[i])

        @pl.when(has_up)
        def _():
            remote(slots.at[line], slots.at[line], xs, rd.at[i]).wait_recv()
            put(acc, slots.at[line])

    term(value_grad, other)
    arrive(sb.at[1 - j], bru.at[1 - j], brd.at[1 - j])
    put(vx_out)
    cross = remote(vx_out, vx_in, xs, xr, other)
    cross.start()
    term(value_grad, me)
    arrive(sb.at[j], bru.at[j], brd.at[j])
    put(vfin)
    share_pair(line - 1)

    term(gate_grad, me)
    put(acc, from_pair(i)())
    arrive(sa, aru, ard)

    def finish_gate(cut):
        gfin[cut, :] = acc[cut, :] * scale

    each_rows(finish_gate)
    store_gate = pltpu.make_async_copy(gfin, gate_out, load_sem.at[0])
    store_gate.start()
    cross.wait_recv()

    def finish_value(cut):
        vfin[cut, :] = (vfin[cut, :] + vx_in[cut, :].astype(F32)) * scale

    each_rows(finish_value)
    store_value = pltpu.make_async_copy(vfin, value_out, load_sem.at[1])
    store_value.start()

    conv_out[...] = csum[pl.ds(0, 4), :] * scale

    @pl.loop(0, n_fs)
    def _(o):
        @pl.loop(1, n_tp)
        def _(step):
            source = (tp + step) % n_tp
            remote(ig_send.at[source, o], ig_recv.at[source, o], ig_ss.at[source, o], ig_rs.at[source, o]).wait_recv()

    for o in range(n_fs):
        total = ig_send[tp, o].astype(F32)
        for step in range(1, n_tp):
            total = total + ig_recv[(tp + step) % n_tp, o].astype(F32)
        ig_sum[:, o * shard : (o + 1) * shard] = total.astype(BF16)
    store_input = pltpu.make_async_copy(ig_sum, ig_out, load_sem.at[2])
    store_input.start()

    value_pair(wv_hbm).wait_send()
    cross.wait_send()

    @pl.loop(0, line)
    def _(d):
        @pl.loop(1, n_tp)
        def _(step):
            tok_copy(d, step).wait_send()

        pair_copy(d).wait_send()
        gate_pair(2 * d, wg_hbm).wait_send()

        @pl.when(has_up & (d <= i))
        def _():
            gate_up(2 * d, wg_hbm).wait_send()
            value_up(2 * d, wv_hbm).wait_send()
            value_up(2 * d + 1, wv_hbm).wait_send()

        @pl.when(has_down & (d >= i))
        def _():
            gate_down(2 * d, wg_hbm).wait_send()
            value_down(2 * d, wv_hbm).wait_send()
            value_down(2 * d + 1, wv_hbm).wait_send()

        @pl.when(d > i)
        def _():
            for jd in range(2):
                remote(sb.at[jd, d], sb.at[jd, d], bu.at[jd, d], bru.at[jd, d]).wait_send()
            remote(sa.at[d], sa.at[d], au.at[d], aru.at[d]).wait_send()

        @pl.when(d < i)
        def _():
            for jd in range(2):
                remote(sb.at[jd, d], sb.at[jd, d], bd.at[jd, d], brd.at[jd, d]).wait_send()
            remote(sa.at[d], sa.at[d], ad.at[d], ard.at[d]).wait_send()

    @pl.loop(0, n_fs)
    def _(o):
        @pl.loop(1, n_tp)
        def _(step):
            share_copy((tp + step) % n_tp, o).wait_send()

    store_gate.wait()
    store_value.wait()
    store_input.wait()


def on_device(
    tokens, gate_pre, value_pre, up_gate_w, up_value_w, conv_weight, conv_bias, hidden_grad
):
    n_fs, n_tp = lax.axis_size("fs"), lax.axis_size("tp")
    line = n_fs // 2
    rows, cols = gate_pre.shape
    own_tok, width = tokens.shape
    shard = up_gate_w.shape[0]
    rounds = n_fs.bit_length() - 1
    assert n_fs == 1 << rounds and line >= rounds + 1 and shard * n_fs == width
    scale = float(rows * n_fs) ** (-0.5)
    any_space = pl.BlockSpec(memory_space=pl.ANY)
    vmem = pl.BlockSpec(memory_space=pltpu.VMEM)
    dma = pltpu.SemaphoreType.DMA
    block = (shard, cols)
    input_grad, gate_out, value_out, conv = pl.pallas_call(
        functools.partial(kernel, line, n_tp, scale),
        out_shape=(
            jax.ShapeDtypeStruct((own_tok, width), BF16),
            jax.ShapeDtypeStruct(block, F32),
            jax.ShapeDtypeStruct(block, F32),
            jax.ShapeDtypeStruct((4, cols), F32),
        ),
        in_specs=[any_space] * 6 + [vmem] * 2,
        out_specs=(any_space, any_space, any_space, vmem),
        scratch_shapes=[
            pltpu.VMEM((n_fs, *block), BF16),
            pltpu.VMEM((n_fs, *block), BF16),
            pltpu.VMEM((own_tok, width), BF16),
            pltpu.VMEM((width, rows), BF16),
            pltpu.VMEM((PAD + rows, cols), BF16),
            pltpu.VMEM((rows, cols), BF16),
            pltpu.VMEM((max(rows, line * shard), cols), BF16),
            pltpu.VMEM((rows + 8, LANES), F32),
            pltpu.VMEM(block, F32),
            pltpu.VMEM(block, F32),
            pltpu.VMEM(block, F32),
            pltpu.VMEM((2, line + 1, *block), BF16),
            pltpu.VMEM((line + 1, *block), BF16),
            pltpu.VMEM((line, *block), BF16),
            pltpu.VMEM(block, BF16),
            pltpu.VMEM(block, BF16),
            pltpu.VMEM((n_tp, n_fs, own_tok, shard), BF16),
            pltpu.VMEM((n_tp, n_fs, own_tok, shard), BF16),
            pltpu.VMEM((own_tok, width), BF16),
            pltpu.VMEM((rounds, 4, cols), F32),
            pltpu.VMEM((8, cols), F32),
            dma((6,)),
            dma((n_tp, line)),
            dma((n_tp, line)),
            *[dma((line,))] * 3,
            dma((n_fs,)),
            dma((n_fs,)),
            dma((n_fs,)),
            dma,
            dma((n_fs,)),
            *[dma((2, line))] * 4,
            *[dma((line,))] * 4,
            *[dma((line,))] * 2,
            dma,
            dma,
            *[dma((n_tp, n_fs))] * 2,
            *[dma((rounds,))] * 2,
        ],
        compiler_params=pltpu.CompilerParams(has_side_effects=True, vmem_limit_bytes=67_000_000),
        name="backward",
    )(
        tokens, gate_pre, value_pre, up_gate_w, up_value_w, hidden_grad,
        conv_weight, conv_bias.reshape(1, cols),
    )
    return (input_grad, gate_out, value_out, conv[:3], conv[3])


def solution(mesh):
    return jax.shard_map(
        on_device,
        mesh=mesh,
        in_specs=(
            P(("fs", "tp"), None),
            P("fs", "tp"),
            P("fs", "tp"),
            P("fs", "tp"),
            P("fs", "tp"),
            P(None, "tp"),
            P("tp"),
            P("fs", "tp"),
        ),
        out_specs=(P(("fs", "tp"), None), P("fs", "tp"), P("fs", "tp"), P(None, "tp"), P("tp")),
        check_vma=False,
    )
```

```python
import functools
import math

import jax
import jax.numpy as jnp
from jax import lax
from jax.experimental import pallas as pl
from jax.experimental.pallas import tpu as pltpu
from jax.sharding import PartitionSpec as P

MESH = pl.DeviceIdType.MESH
F32, BF16 = jnp.float32, jnp.bfloat16
PAD = 16
LANES = 128
SPLIT = 2


def dot_rows(left, right):
    return lax.dot_general(left, right, (((1,), (0,)), ((), ())), preferred_element_type=F32)


def dot_cols(left, right):
    return lax.dot_general(left, right, (((1,), (1,)), ((), ())), preferred_element_type=F32)


def tiles(width, tile, body):
    whole = width // tile

    @pl.loop(0, whole)
    def _(n):
        body(pl.multiple_of(n * tile, tile), tile)

    if width % tile:
        body(whole * tile, width % tile)


def kernel(
    line, n_tp, split, scale,
    tok_hbm, gate_hbm, value_hbm, wg_hbm, wv_hbm, hid_hbm, taps, bias,
    ig_sum, gfin, vfin, conv_out, bias_out,
    wa, wb, tok, tok_t, gst, hst, vst, cgs, acc,
    sb, sa, pair_in, vx_out, vx_in, ig_send, ig_recv, conv_recv, csum,
    load_sem, tok_ss, tok_relay, tok_rs,
    a_up, a_down, ax, ra, b_up, b_down, bx, rb,
    bu, bd, bru, brd, au, ad, aru, ard, qs, qr, xs, xr, ig_ss, ig_rs, cs, cr,
):
    me, tp = lax.axis_index("fs"), lax.axis_index("tp")
    i, j = me // 2, me % 2
    other = 2 * i + 1 - j
    up, down = me + 2, me - 2
    has_up, has_down = i < line - 1, i > 0
    n_fs = 2 * line
    rows = hid_hbm.shape[0]
    cols = hid_hbm.shape[1]
    shard = wg_hbm.shape[0]
    own_tok = tok_hbm.shape[0]
    width = tok_hbm.shape[1]
    rounds = n_fs.bit_length() - 1

    def remote(src, dst, ss, rs, fs=None, to_tp=None):
        where = {"fs": me if fs is None else fs, "tp": tp if to_tp is None else to_tp}
        return pltpu.make_async_remote_copy(
            src_ref=src, dst_ref=dst, send_sem=ss, recv_sem=rs, device_id=where, device_id_type=MESH
        )

    def columns_of(ref, first, count):
        return ref if count == ref.shape[-1] else ref.at[:, pl.ds(first, count)]

    barrier = pltpu.get_barrier_semaphore()

    def greet(fs, to_tp):
        pl.semaphore_signal(barrier, inc=1, device_id={"fs": fs, "tp": to_tp}, device_id_type=MESH)

    def part_a(o, ss, to):
        return remote(wa.at[o], wa.at[o], ss.at[o // 2], ra.at[o], to)

    def part_b(o, ss, to):
        return remote(wb.at[o], wb.at[o], ss.at[o], rb.at[o], to)

    def along(part, o, up_ss, down_ss, go_up, go_down):
        @pl.when(go_up)
        def _():
            part(o, up_ss, up).start()

        @pl.when(go_down)
        def _():
            part(o, down_ss, down).start()

    loads = [
        pltpu.make_async_copy(tok_hbm, tok, load_sem.at[0]),
        pltpu.make_async_copy(columns_of(wv_hbm, split, cols - split), wb.at[me], load_sem.at[1]),
        pltpu.make_async_copy(wg_hbm, columns_of(wa.at[me], split, cols), load_sem.at[2]),
        pltpu.make_async_copy(gate_hbm, gst.at[pl.ds(PAD, rows)], load_sem.at[3]),
        pltpu.make_async_copy(hid_hbm, hst, load_sem.at[4]),
        pltpu.make_async_copy(value_hbm, columns_of(vst.at[pl.ds(0, rows)], 0, cols), load_sem.at[5]),
    ]
    if split:
        loads.insert(1, pltpu.make_async_copy(
            columns_of(wv_hbm, 0, split), columns_of(wa.at[me], 0, split), load_sem.at[6]
        ))
    for load in loads:
        load.start()

    greet(other, tp)

    @pl.when(has_up)
    def _():
        greet(up, tp)

    @pl.when(has_down)
    def _():
        greet(down, tp)

    for r in range(2, rounds):
        greet(me ^ (1 << r), tp)

    @pl.loop(1, n_tp)
    def _(step):
        greet(me, (tp + step) % n_tp)

    met = 1 + (rounds - 2) + (n_tp - 1) + jnp.where(has_up, 1, 0) + jnp.where(has_down, 1, 0)
    pl.semaphore_wait(barrier, met)

    weights = 4 if split else 3
    for load in loads[1:weights]:
        load.wait()
    part_b(me, bx, other).start()
    part_a(me, ax, other).start()
    along(part_a, me, a_up, a_down, has_up, has_down)
    along(part_b, me, b_up, b_down, has_up, has_down)

    loads[0].wait()
    turn = 256

    @pl.loop(0, width // turn)
    def _(n):
        at = pl.multiple_of(n * turn, turn)
        tok_t[pl.ds(at, turn), pl.ds(pl.multiple_of(tp * own_tok, own_tok), own_tok)] = tok[
            :, pl.ds(at, turn)
        ].T

    def tok_piece(d, source):
        return tok_t.at[
            pl.ds(pl.multiple_of(d * 2 * shard, 2 * shard), 2 * shard),
            pl.ds(pl.multiple_of(source * own_tok, own_tok), own_tok),
        ]

    def far(n):
        mirror = 2 * i >= line
        at = jnp.where(mirror, line - 1 - i, i)
        d = line - 1 - n
        d = jnp.where(d > at, d, jnp.where(d == 0, at, d - 1))
        return jnp.where(mirror, line - 1 - d, d)

    def tok_copy(d, source, ss, to):
        return remote(tok_piece(d, source), tok_piece(d, source), ss, tok_rs.at[source, d], to_tp=to)

    core, twin, chips = tp % 2, tp + 1 - 2 * (tp % 2), n_tp // 2

    def on_chip(step):
        return 2 * ((tp // 2 + step) % chips) + core

    @pl.loop(0, line)
    def _(n):
        d = far(n)

        @pl.loop(1, chips)
        def _(step):
            tok_copy(d, tp, tok_ss.at[on_chip(step), d], on_chip(step)).start()

        tok_copy(d, tp, tok_relay.at[tp, d], twin).start()

    def tok_relayed(d):
        @pl.loop(1, chips)
        def _(step):
            source = on_chip(step)
            tok_copy(d, source, tok_relay.at[source, d], twin).wait_recv()
            tok_copy(d, source, tok_relay.at[source, d], twin).start()

    def tok_landed(d):
        @pl.loop(0, chips)
        def _(step):
            source = on_chip(step) + twin - tp
            tok_copy(d, source, tok_relay.at[source, d], twin).wait_recv()

    for load in loads[weights:]:
        load.wait()
    chunk = 64
    root = math.sqrt(2.0 / math.pi)

    def elementwise(at, size):
        cut = pl.ds(at, size)
        gst[pl.ds(0, PAD), cut] = jnp.zeros((PAD, size), BF16)
        w0, w1, w2 = (taps[pl.ds(k, 1), cut] for k in range(3))
        b = bias[:, cut]

        def forward(n, sums):
            r = pl.multiple_of(n * chunk, chunk)
            wide = gst[pl.ds(r, PAD + chunk), cut].astype(F32)
            x0 = wide[PAD:]
            x1 = pltpu.roll(wide, 1, 0)[PAD:]
            x2 = pltpu.roll(wide, 2, 0)[PAD:]
            z = b + w0 * x2 + w1 * x1 + w2 * x0
            sq = z * z
            th = jnp.tanh(root * (z + 0.044715 * (sq * z)))
            cdf = 0.5 * (1.0 + th)
            h = hst[pl.ds(r, chunk), cut].astype(F32)
            v = vst[pl.ds(r, chunk), cut].astype(F32)
            hst[pl.ds(r, chunk), cut] = (h * (z * cdf)).astype(BF16)
            slope = cdf + (0.5 * z) * (1.0 - th * th) * (root + (3.0 * 0.044715 * root) * sq)
            cg = slope * (h * v)
            cgs[pl.ds(r, chunk), pl.ds(0, size)] = cg

            def fold(term):
                return jnp.sum(term.reshape(chunk // 8, 8, size), axis=0)

            return tuple(s + fold(t) for s, t in zip(sums, (cg * x2, cg * x1, cg * x0, cg)))

        zero = jnp.zeros((8, size), F32)
        sums = lax.fori_loop(0, rows // chunk, forward, (zero,) * 4)
        for k in range(4):
            csum[pl.ds(k, 1), cut] = jnp.sum(sums[k], axis=0, keepdims=True)
        cgs[pl.ds(rows, 8), pl.ds(0, size)] = jnp.zeros((8, size), F32)

        @pl.loop(0, rows // chunk)
        def _(n):
            r = pl.multiple_of(n * chunk, chunk)
            wide = cgs[pl.ds(r, chunk + 8), pl.ds(0, size)]
            g1 = pltpu.roll(wide, chunk + 7, 0)[:chunk]
            g2 = pltpu.roll(wide, chunk + 6, 0)[:chunk]
            gst[pl.ds(PAD + r, chunk), cut] = (w2 * wide[:chunk] + w1 * g1 + w0 * g2).astype(BF16)

    tiles(cols, LANES, elementwise)

    def conv_copy(r):
        return remote(csum.at[pl.ds(0, 4)], conv_recv.at[r], cs.at[r], cr.at[r], me ^ (1 << r))

    def conv_add(r):
        conv_copy(r).wait_send()
        conv_copy(r).wait_recv()
        csum[pl.ds(0, 4), :] += conv_recv[r]

    conv_copy(0).start()

    part_b(other, bx, other).wait_recv()
    along(part_b, other, b_up, b_down, has_up, has_down)

    def gather(t):
        low, high = i - t - 1, i + t + 1

        @pl.when(low >= 0)
        def _():
            o = 2 * low + j
            part_a(o, a_up, up).wait_recv()
            along(part_a, o, a_up, a_down, has_up, False)
            part_a(o, ax, other).start()

        @pl.when(high < line)
        def _():
            o = 2 * high + j
            part_a(o, a_down, down).wait_recv()
            along(part_a, o, a_up, a_down, False, has_down)
            part_a(o, ax, other).start()

        for flip in range(2):
            jd = j if flip == 0 else 1 - j

            @pl.when(low >= 0)
            def _():
                o = 2 * low + jd
                part_b(o, b_up, up).wait_recv()
                along(part_b, o, b_up, b_down, has_up, False)

            @pl.when(high < line)
            def _():
                o = 2 * high + jd
                part_b(o, b_down, down).wait_recv()
                along(part_b, o, b_up, b_down, False, has_down)

    wide_a, wide_b = cols + split, cols - split

    def value_cols(at, size):
        return hst[:, pl.ds(at, size)]

    def value_rest(at, size):
        return hst[:, pl.ds(pl.multiple_of(at + split, LANES), size)]

    def gate_cols(at, size):
        return gst[pl.ds(PAD, rows), pl.ds(at, size)]

    def columns(grad, left, first, count):
        def one(at, size):
            to = pl.ds(pl.multiple_of(at + first, LANES), size)
            acc[:, to] = dot_rows(tok_t[left, :], grad(at, size))

        tiles(count, 256, one)

    def term(is_a, o):
        left = pl.ds(pl.multiple_of(o * shard, shard), shard)
        if is_a:
            if split:
                columns(value_cols, left, 0, split)
            columns(gate_cols, left, split, cols)
        else:
            columns(value_rest, left, 0, wide_b)

    step_rows = 16

    def each_rows(body):
        @pl.loop(0, shard // step_rows)
        def _(n):
            body(pl.ds(pl.multiple_of(n * step_rows, step_rows), step_rows))

    def put(dst, *more):
        span = pl.ds(0, dst.shape[-1])

        def body(cut):
            total = acc[cut, span]
            for ref in more:
                total = total + ref[cut, :].astype(F32)
            dst[cut, span] = total.astype(dst.dtype)

        each_rows(body)

    def landing(d, receiver):
        return jnp.where(d == receiver, line, d)

    def hop(is_a, slots, o, d, going_up, ss, rs, extra=None):
        term(is_a, o)
        more = () if extra is None else (extra(),)
        slot = slots.at[d]
        came = has_down if going_up else has_up
        if going_up:
            arrived = remote(slot, slot, ss, rs)
            sent = remote(slot, slot, ss, rs, up)
        else:
            arrived = remote(slot, slot, ss, rs)
            sent = remote(slot, slots.at[landing(d, i - 1)], ss, rs, down)

        @pl.when(came)
        def _():
            arrived.wait_recv()
            put(slot, slot, *more)

        @pl.when(jnp.logical_not(came))
        def _():
            put(slot, *more)

        sent.start()

    def up_row(tt):
        return line - 1 - tt + i

    def down_row(tt):
        return tt - line + 1 + i

    def value_step(tt):
        for jd in range(2):
            @pl.when(tt >= i)
            def _():
                d = up_row(tt)
                hop(False, sb.at[jd], 2 * d + jd, d, True, bu.at[jd, d], bru.at[jd, d])

            @pl.when(tt >= line - 1 - i)
            def _():
                d = down_row(tt)
                hop(False, sb.at[jd], 2 * d + jd, d, False, bd.at[jd, d], brd.at[jd, d])

    def pair_copy(d):
        return remote(vst.at[pl.ds(pl.multiple_of(d * shard, shard), shard), :], pair_in.at[d], qs.at[d], qr.at[d], other)

    def pair_term(n):
        d = far(n)
        term(True, 2 * d + 1 - j)
        put(vst.at[pl.ds(pl.multiple_of(d * shard, shard), shard), :])
        pair_copy(d).start()

    def from_pair(d):
        def get():
            pair_copy(d).wait_recv()
            return pair_in.at[d]

        return get

    def gate_step(tt):
        @pl.when(tt >= i)
        def _():
            d = up_row(tt)
            hop(True, sa, 2 * d + j, d, True, au.at[d], aru.at[d], from_pair(d))

        @pl.when(tt >= line - 1 - i)
        def _():
            d = down_row(tt)
            hop(True, sa, 2 * d + j, d, False, ad.at[d], ard.at[d], from_pair(d))

    def share_copy(k, o):
        return remote(ig_send.at[k, o], ig_recv.at[tp, o], ig_ss.at[k, o], ig_rs.at[tp, o], to_tp=k)

    def share(o):
        @pl.loop(0, n_tp)
        def _(k):
            at = pl.multiple_of(k * own_tok, own_tok)
            here = pl.ds(at, own_tok)
            part = dot_cols(gst[pl.ds(PAD + at, own_tok), :], wa[o, :, pl.ds(split, cols)])
            if split:
                part = part + dot_cols(hst[here, pl.ds(0, split)], wa[o, :, pl.ds(0, split)])
            part = part + dot_cols(hst[here, pl.ds(split, wide_b)], wb[o])
            ig_send[k, o] = part.astype(BF16)

            @pl.when(k != tp)
            def _():
                share_copy(k, o).start()

    def share_line(t):
        for at in (i - t, i + t):
            @pl.when((at >= 0) & (at < line))
            def _():
                share(2 * at + j)

    def share_pair(t, both=True):
        for at in (i - t, i + t)[: 2 if both else 1]:
            @pl.when((at >= 0) & (at < line))
            def _():
                o = 2 * at + 1 - j
                part_a(o, ax, other).wait_recv()
                share(o)

    for n in range(min(2, line)):
        tok_relayed(far(n))
    for n in range(min(2, line)):
        tok_landed(far(n))

    pair_term(0)
    value_step(0)

    @pl.loop(2, line)
    def _(n):
        tok_relayed(far(n))

    @pl.loop(2, line)
    def _(n):
        tok_landed(far(n))

    share(me)

    @pl.loop(1, line - 1)
    def _(tt):
        gather(tt - 1)
        pair_term(tt)

        @pl.when(tt < rounds)
        def _():
            conv_add(tt - 1)
            conv_copy(tt).start()

        value_step(tt)
        share_line(tt)

        @pl.when(tt == 1)
        def _():
            share_pair(0, False)

        @pl.when(tt > 1)
        def _():
            share_pair(tt - 1)

    gate_step(0)
    gather(line - 2)
    pair_term(line - 1)
    conv_add(rounds - 1)
    gate_step(1)
    share_line(line - 1)
    share_pair(line - 2)

    @pl.loop(2, line - 1)
    def _(tt):
        gate_step(tt)

    def arrive(slots, ru, rd, finish):
        low, high = slots.at[i], slots.at[line]

        @pl.when(has_down)
        def _():
            remote(low, low, xs, ru.at[i]).wait_recv()

        @pl.when(has_up)
        def _():
            remote(high, high, xs, rd.at[i]).wait_recv()

        @pl.when(has_down & has_up)
        def _():
            finish(low, high)

        @pl.when(jnp.logical_not(has_up))
        def _():
            finish(low)

        @pl.when(jnp.logical_not(has_down))
        def _():
            finish(high)

    term(False, other)
    arrive(sb.at[1 - j], bru.at[1 - j], brd.at[1 - j], lambda *refs: put(vx_out, *refs))
    cross = remote(vx_out, vx_in, xs, xr, other)
    cross.start()
    term(False, me)
    arrive(sb.at[j], bru.at[j], brd.at[j], lambda *refs: put(columns_of(vfin, split, wide_b), *refs))
    share_pair(line - 1)

    @pl.loop(0, n_fs)
    def _(o):
        @pl.loop(1, n_tp)
        def _(step):
            source = (tp + step) % n_tp
            remote(ig_send.at[source, o], ig_recv.at[source, o], ig_ss.at[source, o], ig_rs.at[source, o]).wait_recv()

    for o in range(n_fs):
        total = ig_send[tp, o].astype(F32)
        for step in range(1, n_tp):
            total = total + ig_recv[(tp + step) % n_tp, o].astype(F32)
        ig_sum[:, o * shard : (o + 1) * shard] = total.astype(BF16)
    conv_out[...] = csum[pl.ds(0, 3), :] * scale
    bias_out[...] = csum[pl.ds(3, 1), :] * scale

    term(True, me)
    put(acc, from_pair(i)())
    cross.wait_recv()

    def finish_value(cut):
        rest = pl.ds(split, wide_b)
        vfin[cut, rest] = (vfin[cut, rest] + vx_in[cut, :].astype(F32)) * scale

    each_rows(finish_value)

    def finish_gate(*refs):
        def body(cut):
            total = acc[cut, :]
            for ref in refs:
                total = total + ref[cut, :].astype(F32)
            total = total * scale
            gfin[cut, :] = total[:, split:]
            if split:
                vfin[cut, pl.ds(0, split)] = total[:, :split]

        each_rows(body)

    arrive(sa, aru, ard, finish_gate)

    part_b(me, bx, other).wait_send()
    cross.wait_send()

    @pl.loop(0, line)
    def _(d):
        @pl.loop(1, chips)
        def _(step):
            source = on_chip(step)
            tok_copy(d, tp, tok_ss.at[source, d], source).wait_send()
            tok_copy(d, source, tok_relay.at[source, d], twin).wait_send()

        tok_copy(d, tp, tok_relay.at[tp, d], twin).wait_send()
        pair_copy(d).wait_send()
        part_a(2 * d, ax, other).wait_send()

        @pl.when(has_up & (d <= i))
        def _():
            part_a(2 * d, a_up, up).wait_send()
            part_b(2 * d, b_up, up).wait_send()
            part_b(2 * d + 1, b_up, up).wait_send()

        @pl.when(has_down & (d >= i))
        def _():
            part_a(2 * d, a_down, down).wait_send()
            part_b(2 * d, b_down, down).wait_send()
            part_b(2 * d + 1, b_down, down).wait_send()

        @pl.when(d > i)
        def _():
            for jd in range(2):
                remote(sb.at[jd, d], sb.at[jd, d], bu.at[jd, d], bru.at[jd, d]).wait_send()
            remote(sa.at[d], sa.at[d], au.at[d], aru.at[d]).wait_send()

        @pl.when(d < i)
        def _():
            for jd in range(2):
                remote(sb.at[jd, d], sb.at[jd, d], bd.at[jd, d], brd.at[jd, d]).wait_send()
            remote(sa.at[d], sa.at[d], ad.at[d], ard.at[d]).wait_send()

    @pl.loop(0, n_fs)
    def _(o):
        @pl.loop(1, n_tp)
        def _(step):
            share_copy((tp + step) % n_tp, o).wait_send()


def on_device(
    tokens, gate_pre, value_pre, up_gate_w, up_value_w, conv_weight, conv_bias, hidden_grad
):
    n_fs, n_tp = lax.axis_size("fs"), lax.axis_size("tp")
    line = n_fs // 2
    rows, cols = gate_pre.shape
    own_tok, width = tokens.shape
    shard = up_gate_w.shape[0]
    rounds = n_fs.bit_length() - 1
    assert n_fs == 1 << rounds and line >= rounds + 1 and shard * n_fs == width
    scale = float(rows * n_fs) ** (-0.5)
    any_space = pl.BlockSpec(memory_space=pl.ANY)
    vmem = pl.BlockSpec(memory_space=pltpu.VMEM)
    dma = pltpu.SemaphoreType.DMA
    split = 0 if cols % LANES else cols * SPLIT // (11 * LANES) * LANES
    block, block_a, block_b = (shard, cols), (shard, cols + split), (shard, cols - split)
    input_grad, gate_out, value_out, conv, bias = pl.pallas_call(
        functools.partial(kernel, line, n_tp, split, scale),
        out_shape=(
            pltpu.VMEM((own_tok, width), BF16),
            pltpu.VMEM(block, F32),
            pltpu.VMEM(block, F32),
            pltpu.VMEM((3, cols), F32),
            pltpu.VMEM((1, cols), F32),
        ),
        in_specs=[any_space] * 6 + [vmem] * 2,
        out_specs=(vmem,) * 5,
        scratch_shapes=[
            pltpu.VMEM((n_fs, *block_a), BF16),
            pltpu.VMEM((n_fs, *block_b), BF16),
            pltpu.VMEM((own_tok, width), BF16),
            pltpu.VMEM((width, rows), BF16),
            pltpu.VMEM((PAD + rows, cols), BF16),
            pltpu.VMEM((rows, cols), BF16),
            pltpu.VMEM((max(rows, line * shard), cols + split), BF16),
            pltpu.VMEM((rows + 8, LANES), F32),
            pltpu.VMEM(block_a, F32),
            pltpu.VMEM((2, line + 1, *block_b), BF16),
            pltpu.VMEM((line + 1, *block_a), BF16),
            pltpu.VMEM((line, *block_a), BF16),
            pltpu.VMEM(block_b, BF16),
            pltpu.VMEM(block_b, BF16),
            pltpu.VMEM((n_tp, n_fs, own_tok, shard), BF16),
            pltpu.VMEM((n_tp, n_fs, own_tok, shard), BF16),
            pltpu.VMEM((rounds, 4, cols), F32),
            pltpu.VMEM((8, cols), F32),
            dma((7,)),
            *[dma((n_tp, line))] * 3,
            *[dma((line,))] * 3,
            dma((n_fs,)),
            dma((n_fs,)),
            dma((n_fs,)),
            dma((n_fs,)),
            dma((n_fs,)),
            *[dma((2, line))] * 4,
            *[dma((line,))] * 4,
            *[dma((line,))] * 2,
            dma,
            dma,
            *[dma((n_tp, n_fs))] * 2,
            *[dma((rounds,))] * 2,
        ],
        compiler_params=pltpu.CompilerParams(
            collective_id=0, has_side_effects=True, vmem_limit_bytes=60_000_000
        ),
        name="backward",
    )(
        tokens, gate_pre, value_pre, up_gate_w, up_value_w, hidden_grad,
        conv_weight, conv_bias.reshape(1, cols),
    )
    return (input_grad, gate_out, value_out, conv, bias.reshape(cols))


def solution(mesh):
    return jax.shard_map(
        on_device,
        mesh=mesh,
        in_specs=(
            P(("fs", "tp"), None),
            P("fs", "tp"),
            P("fs", "tp"),
            P("fs", "tp"),
            P("fs", "tp"),
            P(None, "tp"),
            P("tp"),
            P("fs", "tp"),
        ),
        out_specs=(P(("fs", "tp"), None), P("fs", "tp"), P("fs", "tp"), P(None, "tp"), P("tp")),
        check_vma=False,
    )
```

```python
import functools
import math
from types import SimpleNamespace

import jax
import jax.numpy as jnp
from jax import lax
from jax.experimental import pallas as pl
from jax.experimental.pallas import tpu as pltpu
from jax.sharding import PartitionSpec as P

MESH = pl.DeviceIdType.MESH
F32, BF16 = jnp.float32, jnp.bfloat16
PAD = 16
LANES = 128
SPLIT = 7
GROUPS = 3


def dot_rows(left, right):
    return lax.dot_general(left, right, (((1,), (0,)), ((), ())), preferred_element_type=F32)


def dot_cols(left, right):
    return lax.dot_general(left, right, (((1,), (1,)), ((), ())), preferred_element_type=F32)


def tiles(width, tile, body, first=0):
    whole = width // tile

    @pl.loop(0, whole)
    def _(n):
        body(pl.multiple_of(n * tile + first, LANES), tile)

    if width % tile:
        body(first + whole * tile, width % tile)


def groups_of(cols, split):
    width = split + cols
    if cols % LANES:
        edges = [0, width]
    else:
        edges = [width // LANES * g // GROUPS * LANES for g in range(GROUPS + 1)]
    pieces = []
    for first, last in zip(edges, edges[1:]):
        piece = []
        if first < split:
            piece.append((False, first, 0, min(last, split) - first))
        if last > split:
            at = max(first, split)
            piece.append((True, at - split, at - first, last - at))
        pieces.append((first, last - first, piece))
    return pieces


def kernel(
    line, n_tp, split, pieces, names, scale,
    tok_hbm, gate_hbm, value_hbm, wg_hbm, wv_hbm, hid_hbm, taps, bias,
    ig_sum, gfin, vfin, conv_out, bias_out, *scratch,
):
    own = SimpleNamespace(**dict(zip(names, scratch, strict=True)))
    wa, wb, tok, tok_t, pair_tok, gst, hst, vst = (
        own.wa, own.wb, own.tok, own.tok_t, own.pair_tok, own.gst, own.hst, own.vst
    )
    cgs, acc, csum, conv_recv, load_sem = own.cgs, own.acc, own.csum, own.conv_recv, own.load_sem
    tok_ss, tok_relay, tok_rs = own.tok_ss, own.tok_relay, own.tok_rs
    ig_send, ig_recv = own.ig_send, own.ig_recv
    me, tp = lax.axis_index("fs"), lax.axis_index("tp")
    i, j = me // 2, me % 2
    other = 2 * i + 1 - j
    up, down = me + 2, me - 2
    has_up, has_down = i < line - 1, i > 0
    n_fs = 2 * line
    rows, cols = hid_hbm.shape
    shard = wg_hbm.shape[0]
    own_tok, width = tok_hbm.shape
    rounds = n_fs.bit_length() - 1
    wide_b = cols - split

    def remote(src, dst, ss, rs, fs=None, to_tp=None):
        where = {"fs": me if fs is None else fs, "tp": tp if to_tp is None else to_tp}
        return pltpu.make_async_remote_copy(
            src_ref=src, dst_ref=dst, send_sem=ss, recv_sem=rs, device_id=where, device_id_type=MESH
        )

    def columns_of(ref, first, count):
        return ref if count == ref.shape[-1] else ref.at[:, pl.ds(first, count)]

    barrier = pltpu.get_barrier_semaphore()

    def greet(fs, to_tp):
        pl.semaphore_signal(barrier, inc=1, device_id={"fs": fs, "tp": to_tp}, device_id_type=MESH)

    greet(other, tp)

    @pl.when(has_up)
    def _():
        greet(up, tp)

    @pl.when(has_down)
    def _():
        greet(down, tp)

    for r in range(2, rounds):
        greet(me ^ (1 << r), tp)

    @pl.loop(1, n_tp)
    def _(step):
        greet(me, (tp + step) % n_tp)

    def part_a(o, ss, to):
        return remote(wa.at[o // 2], wa.at[o // 2], ss.at[o // 2], own.ra.at[o // 2], to)

    def part_b(o, ss, to):
        return remote(wb.at[o], wb.at[o], ss.at[o], own.rb.at[o], to)

    a_up, a_down, b_up, b_down, bx = own.a_up, own.a_down, own.b_up, own.b_down, own.bx

    def along(part, o, up_ss, down_ss, go_up, go_down):
        @pl.when(go_up)
        def _():
            part(o, up_ss, up).start()

        @pl.when(go_down)
        def _():
            part(o, down_ss, down).start()

    loads = [
        pltpu.make_async_copy(tok_hbm, tok, load_sem.at[0]),
        pltpu.make_async_copy(columns_of(wv_hbm, split, wide_b), wb.at[me], load_sem.at[1]),
        pltpu.make_async_copy(wg_hbm, columns_of(wa.at[i], split, cols), load_sem.at[2]),
        pltpu.make_async_copy(gate_hbm, gst.at[pl.ds(PAD, rows)], load_sem.at[3]),
        pltpu.make_async_copy(hid_hbm, hst, load_sem.at[4]),
        pltpu.make_async_copy(value_hbm, vst, load_sem.at[5]),
    ]
    if split:
        loads.insert(1, pltpu.make_async_copy(
            columns_of(wv_hbm, 0, split), columns_of(wa.at[i], 0, split), load_sem.at[6]
        ))
    for load in loads:
        load.start()

    met = 1 + (rounds - 2) + (n_tp - 1) + jnp.where(has_up, 1, 0) + jnp.where(has_down, 1, 0)
    pl.semaphore_wait(barrier, met)

    weights = 4 if split else 3
    for load in loads[1:weights]:
        load.wait()
    part_b(me, bx, other).start()
    along(part_a, me, a_up, a_down, has_up, has_down)
    along(part_b, me, b_up, b_down, has_up, has_down)

    loads[0].wait()
    turn = 256

    @pl.loop(0, width // turn)
    def _(n):
        at = pl.multiple_of(n * turn, turn)
        tok_t[pl.ds(at, turn), pl.ds(pl.multiple_of(tp * own_tok, own_tok), own_tok)] = tok[
            :, pl.ds(at, turn)
        ].T

    def tok_piece(d, source):
        return tok_t.at[
            pl.ds(pl.multiple_of(d * 2 * shard, 2 * shard), 2 * shard),
            pl.ds(pl.multiple_of(source * own_tok, own_tok), own_tok),
        ]

    def far(n):
        mirror = 2 * i >= line
        at = jnp.where(mirror, line - 1 - i, i)
        d = line - 1 - n
        d = jnp.where(d > at, d, jnp.where(d == 0, at, d - 1))
        return jnp.where(mirror, line - 1 - d, d)

    def tok_copy(d, source, ss, to):
        return remote(tok_piece(d, source), tok_piece(d, source), ss, tok_rs.at[source, d], to_tp=to)

    core, twin, chips = tp % 2, tp + 1 - 2 * (tp % 2), n_tp // 2

    def on_chip(step):
        return 2 * ((tp // 2 + step) % chips) + core

    @pl.loop(0, line)
    def _(n):
        d = far(n)

        @pl.loop(1, chips)
        def _(step):
            tok_copy(d, tp, tok_ss.at[on_chip(step), d], on_chip(step)).start()

        tok_copy(d, tp, tok_relay.at[tp, d], twin).start()

    def tok_relayed(d):
        @pl.loop(1, chips)
        def _(step):
            source = on_chip(step)
            tok_copy(d, source, tok_relay.at[source, d], twin).wait_recv()
            tok_copy(d, source, tok_relay.at[source, d], twin).start()

    def tok_landed(d):
        @pl.loop(0, chips)
        def _(step):
            source = on_chip(step) + twin - tp
            tok_copy(d, source, tok_relay.at[source, d], twin).wait_recv()

    def pair_piece(d):
        return remote(
            tok_t.at[
                pl.ds(pl.multiple_of((2 * d + 1 - j) * shard, shard), shard),
                pl.ds(pl.multiple_of(tp * own_tok, own_tok), own_tok),
            ],
            pair_tok.at[
                pl.ds(pl.multiple_of(d * shard, shard), shard),
                pl.ds(pl.multiple_of(tp * own_tok, own_tok), own_tok),
            ],
            own.px_ss.at[d], own.px_rs.at[d], other,
        )

    def pair_cols(source, ss, to):
        part = pair_tok.at[:, pl.ds(pl.multiple_of(source * own_tok, own_tok), own_tok)]
        return remote(part, part, ss, own.pt_rs.at[source], to_tp=to)

    def pair_tokens_out():
        @pl.loop(0, line)
        def _(d):
            pair_piece(d).wait_recv()

        @pl.loop(1, chips)
        def _(step):
            pair_cols(tp, own.pt_ss.at[on_chip(step)], on_chip(step)).start()

        pair_cols(tp, own.pt_relay.at[tp], twin).start()

    def pair_tokens_in():
        @pl.loop(1, chips)
        def _(step):
            source = on_chip(step)
            pair_cols(source, own.pt_relay.at[source], twin).wait_recv()
            pair_cols(source, own.pt_relay.at[source], twin).start()

        @pl.loop(0, chips)
        def _(step):
            source = on_chip(step) + twin - tp
            pair_cols(source, own.pt_relay.at[source], twin).wait_recv()

    @pl.loop(0, line)
    def _(d):
        pair_piece(d).start()

    for load in loads[weights:]:
        load.wait()
    chunk = 64
    root = math.sqrt(2.0 / math.pi)

    def elementwise(at, size):
        cut = pl.ds(at, size)
        gst[pl.ds(0, PAD), cut] = jnp.zeros((PAD, size), BF16)
        w0, w1, w2 = (taps[pl.ds(k, 1), cut] for k in range(3))
        b = bias[cut].reshape(1, size)

        def forward(n, sums):
            r = pl.multiple_of(n * chunk, chunk)
            wide = gst[pl.ds(r, PAD + chunk), cut].astype(F32)
            x0 = wide[PAD:]
            x1 = pltpu.roll(wide, 1, 0)[PAD:]
            x2 = pltpu.roll(wide, 2, 0)[PAD:]
            z = b + w0 * x2 + w1 * x1 + w2 * x0
            sq = z * z
            th = jnp.tanh(root * (z + 0.044715 * (sq * z)))
            cdf = 0.5 * (1.0 + th)
            h = hst[pl.ds(r, chunk), cut].astype(F32)
            v = vst[pl.ds(r, chunk), cut].astype(F32)
            hst[pl.ds(r, chunk), cut] = (h * (z * cdf)).astype(BF16)
            slope = cdf + (0.5 * z) * (1.0 - th * th) * (root + (3.0 * 0.044715 * root) * sq)
            cg = slope * (h * v)
            cgs[pl.ds(r, chunk), pl.ds(0, size)] = cg

            def fold(term):
                return jnp.sum(term.reshape(chunk // 8, 8, size), axis=0)

            return tuple(s + fold(t) for s, t in zip(sums, (cg * x2, cg * x1, cg * x0, cg)))

        zero = jnp.zeros((8, size), F32)
        sums = lax.fori_loop(0, rows // chunk, forward, (zero,) * 4)
        for k in range(4):
            csum[pl.ds(k, 1), cut] = jnp.sum(sums[k], axis=0, keepdims=True)
        cgs[pl.ds(rows, 8), pl.ds(0, size)] = jnp.zeros((8, size), F32)

        @pl.loop(0, rows // chunk)
        def _(n):
            r = pl.multiple_of(n * chunk, chunk)
            wide = cgs[pl.ds(r, chunk + 8), pl.ds(0, size)]
            g1 = pltpu.roll(wide, chunk + 7, 0)[:chunk]
            g2 = pltpu.roll(wide, chunk + 6, 0)[:chunk]
            gst[pl.ds(PAD + r, chunk), cut] = (w2 * wide[:chunk] + w1 * g1 + w0 * g2).astype(BF16)

    def grad_ref(is_gate, at, size):
        ref = gst.at[pl.ds(PAD, rows)] if is_gate else hst
        return columns_of(ref, at, size)

    def grad_copies(g):
        _, _, segments = pieces[g]
        into = getattr(own, f"pg{g}")
        return [
            remote(
                grad_ref(is_gate, at, size), columns_of(into, to, size),
                own.g_ss.at[g, n], own.g_rs.at[g, n], other,
            )
            for n, (is_gate, at, to, size) in enumerate(segments)
        ]

    ready = 0
    for g, (_, _, segments) in enumerate(pieces):
        need = max(at + size for _, at, _, size in segments)
        if need > ready:
            tiles(need - ready, LANES, elementwise, ready)
            ready = need
        for copy in grad_copies(g):
            copy.start()
    if ready < cols:
        tiles(cols - ready, LANES, elementwise, ready)

    def conv_copy(r):
        return remote(csum.at[pl.ds(0, 4)], conv_recv.at[r], own.cs.at[r], own.cr.at[r], me ^ (1 << r))

    def conv_add(r):
        conv_copy(r).wait_send()
        conv_copy(r).wait_recv()
        csum[pl.ds(0, 4), :] += conv_recv[r]

    turns = [*range(1, rounds), 0]
    conv_copy(turns[0]).start()

    part_b(other, bx, other).wait_recv()
    along(part_b, other, b_up, b_down, has_up, has_down)

    def gather(t):
        low, high = i - t - 1, i + t + 1

        @pl.when(low >= 0)
        def _():
            o = 2 * low + j
            part_a(o, a_up, up).wait_recv()
            along(part_a, o, a_up, a_down, has_up, False)

        @pl.when(high < line)
        def _():
            o = 2 * high + j
            part_a(o, a_down, down).wait_recv()
            along(part_a, o, a_up, a_down, False, has_down)

        for flip in range(2):
            jd = j if flip == 0 else 1 - j

            @pl.when(low >= 0)
            def _():
                o = 2 * low + jd
                part_b(o, b_up, up).wait_recv()
                along(part_b, o, b_up, b_down, has_up, False)

            @pl.when(high < line)
            def _():
                o = 2 * high + jd
                part_b(o, b_down, down).wait_recv()
                along(part_b, o, b_up, b_down, False, has_down)

    def left_rows(o):
        return pl.ds(pl.multiple_of(o * shard, shard), shard)

    def term_b(o):
        def one(at, size):
            grad = hst[:, pl.ds(pl.multiple_of(at + split, LANES), size)]
            acc[:, pl.ds(at, size)] = dot_rows(tok_t[left_rows(o), :], grad)

        tiles(wide_b, 256, one)

    def term_a(g, d):
        from_pair = getattr(own, f"pg{g}")
        for is_gate, first, to, count in pieces[g][2]:
            def one(at, size):
                cut = pl.ds(at, size)
                if is_gate:
                    grad = gst[pl.ds(PAD, rows), pl.ds(pl.multiple_of(at - to + first, LANES), size)]
                else:
                    grad = hst[:, pl.ds(pl.multiple_of(at - to + first, LANES), size)]
                total = dot_rows(tok_t[left_rows(2 * d + j), :], grad)
                acc[:, cut] = total + dot_rows(pair_tok[left_rows(d), :], from_pair[:, cut])

            tiles(count, 256, one, to)

    step_rows = 16

    def each_rows(body):
        @pl.loop(0, shard // step_rows)
        def _(n):
            body(pl.ds(pl.multiple_of(n * step_rows, step_rows), step_rows))

    def put(dst, *more):
        span = pl.ds(0, dst.shape[-1])

        def body(cut):
            total = acc[cut, span]
            for ref in more:
                total = total + ref[cut, :].astype(F32)
            dst[cut, span] = total.astype(dst.dtype)

        each_rows(body)

    def unit(w, jd=0):
        if w == 0:
            return own.sb.at[jd], own.sb_ss.at[jd], own.sb_rs.at[jd], lambda d: term_b(2 * d + jd)
        return getattr(own, f"sa{w - 1}"), own.sa_ss.at[w - 1], own.sa_rs.at[w - 1], lambda d: term_a(w - 1, d)

    def level(w, h, jd=0):
        slots, ss, rs, term = unit(w, jd)
        going_up, going_down = i == h, i == line - 1 - h

        @pl.when(going_up | going_down)
        def _():
            @pl.loop(0, line - 1 - h)
            def _(n):
                d = jnp.where(going_up, line - 1 - n, n)
                ahead = jnp.where(going_up, i + 1, i - 1)
                to = jnp.where(going_down & (d == ahead), line, d)
                slot = slots.at[d]
                term(d)
                if h:
                    remote(slot, slot, ss.at[d], rs.at[d]).wait_recv()
                    put(slot, slot)
                else:
                    put(slot)
                remote(slot, slots.at[to], ss.at[d], rs.at[to], 2 * ahead + j).start()

    def arrive(w, jd, finish):
        slots, ss, rs, term = unit(w, jd)
        low, high = slots.at[i], slots.at[line]
        term(i)

        @pl.when(has_down)
        def _():
            remote(low, low, ss.at[i], rs.at[i]).wait_recv()

        @pl.when(has_up)
        def _():
            remote(high, high, ss.at[i], rs.at[line]).wait_recv()

        @pl.when(has_down & has_up)
        def _():
            finish(low, high)

        @pl.when(jnp.logical_not(has_up))
        def _():
            finish(low)

        @pl.when(jnp.logical_not(has_down))
        def _():
            finish(high)

    def share_copy(k, o):
        return remote(ig_send.at[k, o], ig_recv.at[tp, o], own.ig_ss.at[k, o], own.ig_rs.at[tp, o], to_tp=k)

    def share(at, column):
        o = 2 * at + column

        @pl.loop(1, n_tp + 1)
        def _(step):
            k = (tp + step) % n_tp
            start = pl.multiple_of(k * own_tok, own_tok)
            here = pl.ds(start, own_tok)
            part = dot_cols(hst[here, pl.ds(split, wide_b)], wb[o])
            if column is j:
                part = part + dot_cols(gst[pl.ds(PAD + start, own_tok), :], wa[at, :, pl.ds(split, cols)])
                if split:
                    part = part + dot_cols(hst[here, pl.ds(0, split)], wa[at, :, pl.ds(0, split)])
            ig_send[k, o] = part.astype(BF16)

            @pl.when(k != tp)
            def _():
                share_copy(k, o).start()

    def share_far(t):
        for at in (i - t, i + t):
            @pl.when((at >= 0) & (at < line))
            def _():
                share(at, j)
                share(at, 1 - j)

    def pair_share_copy(k):
        return remote(own.pi_send.at[k], own.pi_recv.at[tp], own.pi_ss.at[k], own.pi_rs.at[tp], to_tp=k)

    def pair_shares():
        @pl.loop(1, n_tp + 1)
        def _(step):
            k = (tp + step) % n_tp
            here = pl.ds(pl.multiple_of(k * own_tok, own_tok), own_tok)

            @pl.loop(0, line)
            def _(at):
                part = None
                for g, (first, size, _) in enumerate(pieces):
                    one = dot_cols(getattr(own, f"pg{g}")[here, :], wa[at, :, pl.ds(first, size)])
                    part = one if part is None else part + one
                own.pi_send[k, at] = part.astype(BF16)

            @pl.when(k != tp)
            def _():
                pair_share_copy(k).start()

    back = remote(own.ret_out, own.ret_in, own.ret_ss, own.ret_rs, other)

    def pair_shares_back():
        @pl.loop(1, n_tp)
        def _(step):
            source = (tp + step) % n_tp
            remote(own.pi_send.at[source], own.pi_recv.at[source], own.pi_ss.at[source], own.pi_rs.at[source]).wait_recv()

        @pl.loop(0, line)
        def _(at):
            total = own.pi_send[tp, at].astype(F32)
            for step in range(1, n_tp):
                total = total + own.pi_recv[(tp + step) % n_tp, at].astype(F32)
            own.ret_out[at] = total.astype(BF16)

        back.start()

    def finish_piece(g):
        def finish(*refs):
            def body(cut):
                total = acc[cut, pl.ds(0, pieces[g][1])]
                for ref in refs:
                    total = total + ref[cut, :].astype(F32)
                total = total * scale
                for is_gate, at, to, size in pieces[g][2]:
                    (gfin if is_gate else vfin)[cut, pl.ds(at, size)] = total[:, to : to + size]

            each_rows(body)

        arrive(g + 1, 0, finish)

    @pl.loop(0, line)
    def _(n):
        tok_relayed(far(n))

    pair_tokens_out()

    @pl.loop(0, line)
    def _(n):
        tok_landed(far(n))

    waves = len(pieces) + 1
    cross = remote(own.vx_out, own.vx_in, own.xs, own.xr, other)
    for s in range(waves + line - 2):
        for w in range(waves):
            if w and s == w:
                if w == 1:
                    pair_tokens_in()
                for copy in grad_copies(w - 1):
                    copy.wait_recv()
            if 0 <= s - w < line - 1:
                for jd in range(2 if w == 0 else 1):
                    level(w, s - w, jd)
        if s == 0:
            share(i, j)
            share(i, 1 - j)
        if s < line - 1:
            gather(s)
            share_far(s + 1)
        if s % 2 == 0 and s // 2 < rounds:
            conv_add(turns[s // 2])
            if s // 2 + 1 < rounds:
                conv_copy(turns[s // 2 + 1]).start()
        if s == max(waves - 1, line - 2):
            pair_shares()
        if s == line - 1:
            for mine in (False, True):
                column = j if mine else 1 - j
                finish = (
                    (lambda *refs: put(columns_of(vfin, split, wide_b), *refs))
                    if mine
                    else (lambda *refs: put(own.vx_out, *refs))
                )
                arrive(0, column, finish)
                if not mine:
                    cross.start()
        g = s - line
        if 0 <= g < len(pieces) - 1:
            finish_piece(g)

    conv_out[...] = csum[pl.ds(0, 3), :] * scale
    bias_out[...] = (csum[pl.ds(3, 1), :] * scale).reshape(cols)
    pair_shares_back()
    for g in range(max(0, waves - 2), len(pieces)):
        finish_piece(g)
    cross.wait_recv()

    def finish_value(cut):
        rest = pl.ds(split, wide_b)
        vfin[cut, rest] = (vfin[cut, rest] + own.vx_in[cut, :].astype(F32)) * scale

    each_rows(finish_value)

    @pl.loop(0, n_fs)
    def _(o):
        @pl.loop(1, n_tp)
        def _(step):
            source = (tp + step) % n_tp
            remote(
                ig_send.at[source, o], ig_recv.at[source, o], own.ig_ss.at[source, o], own.ig_rs.at[source, o]
            ).wait_recv()

    back.wait_recv()
    for o in range(n_fs):
        total = ig_send[tp, o].astype(F32)
        for step in range(1, n_tp):
            total = total + ig_recv[(tp + step) % n_tp, o].astype(F32)
        total = total + jnp.where(o % 2 != j, own.ret_in[o // 2].astype(F32), 0.0)
        ig_sum[:, o * shard : (o + 1) * shard] = total.astype(BF16)

    part_b(me, bx, other).wait_send()
    cross.wait_send()
    back.wait_send()
    for g in range(len(pieces)):
        for copy in grad_copies(g):
            copy.wait_send()
    pair_cols(tp, own.pt_relay.at[tp], twin).wait_send()

    @pl.loop(1, chips)
    def _(step):
        source = on_chip(step)
        pair_cols(tp, own.pt_ss.at[source], source).wait_send()
        pair_cols(source, own.pt_relay.at[source], twin).wait_send()

    @pl.loop(1, n_tp)
    def _(step):
        pair_share_copy((tp + step) % n_tp).wait_send()

    @pl.loop(0, line)
    def _(d):
        @pl.loop(1, chips)
        def _(step):
            source = on_chip(step)
            tok_copy(d, tp, tok_ss.at[source, d], source).wait_send()
            tok_copy(d, source, tok_relay.at[source, d], twin).wait_send()

        tok_copy(d, tp, tok_relay.at[tp, d], twin).wait_send()
        pair_piece(d).wait_send()

        @pl.when(has_up & (d <= i))
        def _():
            part_a(2 * d, a_up, up).wait_send()
            part_b(2 * d, b_up, up).wait_send()
            part_b(2 * d + 1, b_up, up).wait_send()

        @pl.when(has_down & (d >= i))
        def _():
            part_a(2 * d, a_down, down).wait_send()
            part_b(2 * d, b_down, down).wait_send()
            part_b(2 * d + 1, b_down, down).wait_send()

        @pl.when(d != i)
        def _():
            for w in range(waves):
                for jd in range(2 if w == 0 else 1):
                    slots, ss, rs, _ = unit(w, jd)
                    remote(slots.at[d], slots.at[d], ss.at[d], rs.at[d]).wait_send()

    @pl.loop(0, n_fs)
    def _(o):
        @pl.loop(1, n_tp)
        def _(step):
            share_copy((tp + step) % n_tp, o).wait_send()


def scratch_of(line, n_tp, split, pieces, rows, cols, own_tok, width, shard, rounds):
    n_fs, parts, wide_b = 2 * line, len(pieces), cols - split
    dma = pltpu.SemaphoreType.DMA
    widest = max([wide_b] + [size for _, size, _ in pieces])
    table = dict(
        wa=pltpu.VMEM((line, shard, cols + split), BF16),
        wb=pltpu.VMEM((n_fs, shard, wide_b), BF16),
        tok=pltpu.VMEM((own_tok, width), BF16),
        tok_t=pltpu.VMEM((width, rows), BF16),
        pair_tok=pltpu.VMEM((line * shard, rows), BF16),
        gst=pltpu.VMEM((PAD + rows, cols), BF16),
        hst=pltpu.VMEM((rows, cols), BF16),
        vst=pltpu.VMEM((rows, cols), BF16),
        cgs=pltpu.VMEM((rows + 8, LANES), F32),
        acc=pltpu.VMEM((shard, widest), F32),
        sb=pltpu.VMEM((2, line + 1, shard, wide_b), BF16),
        vx_out=pltpu.VMEM((shard, wide_b), BF16),
        vx_in=pltpu.VMEM((shard, wide_b), BF16),
        ig_send=pltpu.VMEM((n_tp, n_fs, own_tok, shard), BF16),
        ig_recv=pltpu.VMEM((n_tp, n_fs, own_tok, shard), BF16),
        pi_send=pltpu.VMEM((n_tp, line, own_tok, shard), BF16),
        pi_recv=pltpu.VMEM((n_tp, line, own_tok, shard), BF16),
        ret_out=pltpu.VMEM((line, own_tok, shard), BF16),
        ret_in=pltpu.VMEM((line, own_tok, shard), BF16),
        conv_recv=pltpu.VMEM((rounds, 4, cols), F32),
        csum=pltpu.VMEM((8, cols), F32),
        load_sem=dma((7,)),
        tok_ss=dma((n_tp, line)), tok_relay=dma((n_tp, line)), tok_rs=dma((n_tp, line)),
        px_ss=dma((line,)), px_rs=dma((line,)),
        pt_ss=dma((n_tp,)), pt_relay=dma((n_tp,)), pt_rs=dma((n_tp,)),
        a_up=dma((line,)), a_down=dma((line,)), ra=dma((line,)),
        b_up=dma((n_fs,)), b_down=dma((n_fs,)), bx=dma((n_fs,)), rb=dma((n_fs,)),
        g_ss=dma((parts, 2)), g_rs=dma((parts, 2)),
        sb_ss=dma((2, line)), sb_rs=dma((2, line + 1)),
        sa_ss=dma((parts, line)), sa_rs=dma((parts, line + 1)),
        xs=dma, xr=dma, ret_ss=dma, ret_rs=dma,
        ig_ss=dma((n_tp, n_fs)), ig_rs=dma((n_tp, n_fs)),
        pi_ss=dma((n_tp,)), pi_rs=dma((n_tp,)),
        cs=dma((rounds,)), cr=dma((rounds,)),
    )
    for g, (_, size, _) in enumerate(pieces):
        table[f"pg{g}"] = pltpu.VMEM((rows, size), BF16)
        table[f"sa{g}"] = pltpu.VMEM((line + 1, shard, size), BF16)
    return table


def on_device(
    tokens, gate_pre, value_pre, up_gate_w, up_value_w, conv_weight, conv_bias, hidden_grad
):
    n_fs, n_tp = lax.axis_size("fs"), lax.axis_size("tp")
    line = n_fs // 2
    rows, cols = gate_pre.shape
    own_tok, width = tokens.shape
    shard = up_gate_w.shape[0]
    rounds = n_fs.bit_length() - 1
    assert n_fs == 1 << rounds and line >= max(4, rounds) and shard * n_fs == width and n_tp % 2 == 0
    scale = float(rows * n_fs) ** (-0.5)
    split = 0 if cols % LANES else cols * SPLIT // (11 * LANES) * LANES
    pieces = groups_of(cols, split)
    table = scratch_of(line, n_tp, split, pieces, rows, cols, own_tok, width, shard, rounds)
    any_space = pl.BlockSpec(memory_space=pl.ANY)
    vmem = pl.BlockSpec(memory_space=pltpu.VMEM)
    input_grad, gate_out, value_out, conv, bias = pl.pallas_call(
        functools.partial(kernel, line, n_tp, split, pieces, tuple(table), scale),
        out_shape=(
            pltpu.VMEM((own_tok, width), BF16),
            pltpu.VMEM((shard, cols), F32),
            pltpu.VMEM((shard, cols), F32),
            pltpu.VMEM((3, cols), F32),
            pltpu.VMEM((cols,), F32),
        ),
        in_specs=[any_space] * 6 + [vmem] * 2,
        out_specs=(vmem,) * 5,
        scratch_shapes=list(table.values()),
        compiler_params=pltpu.CompilerParams(
            collective_id=0, has_side_effects=True, vmem_limit_bytes=61_000_000
        ),
        name="backward",
    )(
        tokens, gate_pre, value_pre, up_gate_w, up_value_w, hidden_grad,
        conv_weight, conv_bias,
    )
    return (input_grad, gate_out, value_out, conv, bias)


def solution(mesh):
    return jax.shard_map(
        on_device,
        mesh=mesh,
        in_specs=(
            P(("fs", "tp"), None),
            P("fs", "tp"),
            P("fs", "tp"),
            P("fs", "tp"),
            P("fs", "tp"),
            P(None, "tp"),
            P("tp"),
            P("fs", "tp"),
        ),
        out_specs=(P(("fs", "tp"), None), P("fs", "tp"), P("fs", "tp"), P(None, "tp"), P("tp")),
        check_vma=False,
    )
```

```python
import functools
import math
from types import SimpleNamespace

import jax
import jax.numpy as jnp
from jax import lax
from jax.experimental import pallas as pl
from jax.experimental.pallas import tpu as pltpu
from jax.sharding import PartitionSpec as P

MESH = pl.DeviceIdType.MESH
F32, BF16 = jnp.float32, jnp.bfloat16
PAD = 16
LANES = 128
SPLIT = 7
GROUPS = 3


def dot_rows(left, right):
    return lax.dot_general(left, right, (((1,), (0,)), ((), ())), preferred_element_type=F32)


def dot_cols(left, right):
    return lax.dot_general(left, right, (((1,), (1,)), ((), ())), preferred_element_type=F32)


def tiles(width, tile, body, first=0):
    whole = width // tile

    @pl.loop(0, whole)
    def _(n):
        body(pl.multiple_of(n * tile + first, LANES), tile)

    if width % tile:
        body(first + whole * tile, width % tile)


def groups_of(cols, split):
    width = split + cols
    if cols % LANES:
        edges = [0, width]
    else:
        edges = [width // LANES * g // GROUPS * LANES for g in range(GROUPS + 1)]
    pieces = []
    for first, last in zip(edges, edges[1:]):
        piece = []
        if first < split:
            piece.append((False, first, 0, min(last, split) - first))
        if last > split:
            at = max(first, split)
            piece.append((True, at - split, at - first, last - at))
        pieces.append((first, last - first, piece))
    return pieces


def kernel(
    line, n_tp, split, pieces, names, scale,
    tok_hbm, gate_hbm, value_hbm, wg_hbm, wv_hbm, hid_hbm, taps, bias,
    ig_sum, gfin, vfin, conv_out, bias_out, *scratch,
):
    own = SimpleNamespace(**dict(zip(names, scratch, strict=True)))
    wa, wb, tok, tok_t, pair_tok, gst, hst, vst = (
        own.wa, own.wb, own.tok, own.tok_t, own.pair_tok, own.gst, own.hst, own.vst
    )
    cgs, acc, csum, conv_recv, load_sem = own.cgs, own.acc, own.csum, own.conv_recv, own.load_sem
    tok_ss, tok_relay, tok_rs = own.tok_ss, own.tok_relay, own.tok_rs
    ig_send, ig_recv = own.ig_send, own.ig_recv
    me, tp = lax.axis_index("fs"), lax.axis_index("tp")
    i, j = me // 2, me % 2
    other = 2 * i + 1 - j
    up, down = me + 2, me - 2
    has_up, has_down = i < line - 1, i > 0
    n_fs = 2 * line
    rows, cols = hid_hbm.shape
    shard = wg_hbm.shape[0]
    own_tok, width = tok_hbm.shape
    rounds = n_fs.bit_length() - 1
    wide_b = cols - split

    def remote(src, dst, ss, rs, fs=None, to_tp=None):
        where = {"fs": me if fs is None else fs, "tp": tp if to_tp is None else to_tp}
        return pltpu.make_async_remote_copy(
            src_ref=src, dst_ref=dst, send_sem=ss, recv_sem=rs, device_id=where, device_id_type=MESH
        )

    def columns_of(ref, first, count):
        return ref if count == ref.shape[-1] else ref.at[:, pl.ds(first, count)]

    barrier = pltpu.get_barrier_semaphore()

    def greet(fs, to_tp):
        pl.semaphore_signal(barrier, inc=1, device_id={"fs": fs, "tp": to_tp}, device_id_type=MESH)

    greet(other, tp)

    @pl.when(has_up)
    def _():
        greet(up, tp)

    @pl.when(has_down)
    def _():
        greet(down, tp)

    for r in range(2, rounds):
        greet(me ^ (1 << r), tp)

    @pl.loop(1, n_tp)
    def _(step):
        greet(me, (tp + step) % n_tp)

    def part_a(o, ss, to):
        return remote(wa.at[o // 2], wa.at[o // 2], ss.at[o // 2], own.ra.at[o // 2], to)

    def part_b(o, ss, to):
        return remote(wb.at[o], wb.at[o], ss.at[o], own.rb.at[o], to)

    a_up, a_down, b_up, b_down, bx = own.a_up, own.a_down, own.b_up, own.b_down, own.bx

    def along(part, o, up_ss, down_ss, go_up, go_down):
        @pl.when(go_up)
        def _():
            part(o, up_ss, up).start()

        @pl.when(go_down)
        def _():
            part(o, down_ss, down).start()

    loads = [
        pltpu.make_async_copy(tok_hbm, tok, load_sem.at[0]),
        pltpu.make_async_copy(columns_of(wv_hbm, split, wide_b), wb.at[me], load_sem.at[1]),
        pltpu.make_async_copy(wg_hbm, columns_of(wa.at[i], split, cols), load_sem.at[2]),
        pltpu.make_async_copy(gate_hbm, gst.at[pl.ds(PAD, rows)], load_sem.at[3]),
        pltpu.make_async_copy(hid_hbm, hst, load_sem.at[4]),
        pltpu.make_async_copy(value_hbm, vst, load_sem.at[5]),
    ]
    if split:
        loads.insert(1, pltpu.make_async_copy(
            columns_of(wv_hbm, 0, split), columns_of(wa.at[i], 0, split), load_sem.at[6]
        ))
    for load in loads:
        load.start()

    met = 1 + (rounds - 2) + (n_tp - 1) + jnp.where(has_up, 1, 0) + jnp.where(has_down, 1, 0)
    pl.semaphore_wait(barrier, met)

    weights = 4 if split else 3
    for load in loads[1:weights]:
        load.wait()
    part_b(me, bx, other).start()
    along(part_a, me, a_up, a_down, has_up, has_down)
    along(part_b, me, b_up, b_down, has_up, has_down)

    loads[0].wait()
    turn = 256

    @pl.loop(0, width // turn)
    def _(n):
        at = pl.multiple_of(n * turn, turn)
        tok_t[pl.ds(at, turn), pl.ds(pl.multiple_of(tp * own_tok, own_tok), own_tok)] = tok[
            :, pl.ds(at, turn)
        ].T

    def tok_piece(d, source):
        return tok_t.at[
            pl.ds(pl.multiple_of(d * 2 * shard, 2 * shard), 2 * shard),
            pl.ds(pl.multiple_of(source * own_tok, own_tok), own_tok),
        ]

    def far(n):
        mirror = 2 * i >= line
        at = jnp.where(mirror, line - 1 - i, i)
        d = line - 1 - n
        d = jnp.where(d > at, d, jnp.where(d == 0, at, d - 1))
        return jnp.where(mirror, line - 1 - d, d)

    def tok_copy(d, source, ss, to):
        return remote(tok_piece(d, source), tok_piece(d, source), ss, tok_rs.at[source, d], to_tp=to)

    core, twin, chips = tp % 2, tp + 1 - 2 * (tp % 2), n_tp // 2

    def on_chip(step):
        return 2 * ((tp // 2 + step) % chips) + core

    @pl.loop(0, line)
    def _(n):
        d = far(n)

        @pl.loop(1, chips)
        def _(step):
            tok_copy(d, tp, tok_ss.at[on_chip(step), d], on_chip(step)).start()

        tok_copy(d, tp, tok_relay.at[tp, d], twin).start()

    def tok_relayed(d):
        @pl.loop(1, chips)
        def _(step):
            source = on_chip(step)
            tok_copy(d, source, tok_relay.at[source, d], twin).wait_recv()
            tok_copy(d, source, tok_relay.at[source, d], twin).start()

    def tok_landed(d):
        @pl.loop(0, chips)
        def _(step):
            source = on_chip(step) + twin - tp
            tok_copy(d, source, tok_relay.at[source, d], twin).wait_recv()

    def pair_piece(d):
        return remote(
            tok_t.at[
                pl.ds(pl.multiple_of((2 * d + 1 - j) * shard, shard), shard),
                pl.ds(pl.multiple_of(tp * own_tok, own_tok), own_tok),
            ],
            pair_tok.at[
                pl.ds(pl.multiple_of(d * shard, shard), shard),
                pl.ds(pl.multiple_of(tp * own_tok, own_tok), own_tok),
            ],
            own.px_ss.at[d], own.px_rs.at[d], other,
        )

    def pair_cols(source, ss, to):
        part = pair_tok.at[:, pl.ds(pl.multiple_of(source * own_tok, own_tok), own_tok)]
        return remote(part, part, ss, own.pt_rs.at[source], to_tp=to)

    def pair_tokens_out():
        @pl.loop(0, line)
        def _(d):
            pair_piece(d).wait_recv()

        @pl.loop(1, chips)
        def _(step):
            pair_cols(tp, own.pt_ss.at[on_chip(step)], on_chip(step)).start()

        pair_cols(tp, own.pt_relay.at[tp], twin).start()

    def pair_tokens_in():
        @pl.loop(1, chips)
        def _(step):
            source = on_chip(step)
            pair_cols(source, own.pt_relay.at[source], twin).wait_recv()
            pair_cols(source, own.pt_relay.at[source], twin).start()

        @pl.loop(0, chips)
        def _(step):
            source = on_chip(step) + twin - tp
            pair_cols(source, own.pt_relay.at[source], twin).wait_recv()

    @pl.loop(0, line)
    def _(d):
        pair_piece(d).start()

    for load in loads[weights:]:
        load.wait()
    chunk = 64
    root = math.sqrt(2.0 / math.pi)

    def elementwise(at, size):
        cut = pl.ds(at, size)
        gst[pl.ds(0, PAD), cut] = jnp.zeros((PAD, size), BF16)
        w0, w1, w2 = (taps[pl.ds(k, 1), cut] for k in range(3))
        b = bias[cut].reshape(1, size)

        def forward(n, sums):
            r = pl.multiple_of(n * chunk, chunk)
            wide = gst[pl.ds(r, PAD + chunk), cut].astype(F32)
            x0 = wide[PAD:]
            x1 = pltpu.roll(wide, 1, 0)[PAD:]
            x2 = pltpu.roll(wide, 2, 0)[PAD:]
            z = b + w0 * x2 + w1 * x1 + w2 * x0
            sq = z * z
            th = jnp.tanh(root * (z + 0.044715 * (sq * z)))
            cdf = 0.5 * (1.0 + th)
            h = hst[pl.ds(r, chunk), cut].astype(F32)
            v = vst[pl.ds(r, chunk), cut].astype(F32)
            hst[pl.ds(r, chunk), cut] = (h * (z * cdf)).astype(BF16)
            slope = cdf + (0.5 * z) * (1.0 - th * th) * (root + (3.0 * 0.044715 * root) * sq)
            cg = slope * (h * v)
            cgs[pl.ds(r, chunk), pl.ds(0, size)] = cg

            def fold(term):
                return jnp.sum(term.reshape(chunk // 8, 8, size), axis=0)

            return tuple(s + fold(t) for s, t in zip(sums, (cg * x2, cg * x1, cg * x0, cg)))

        zero = jnp.zeros((8, size), F32)
        sums = lax.fori_loop(0, rows // chunk, forward, (zero,) * 4)
        for k in range(4):
            csum[pl.ds(k, 1), cut] = jnp.sum(sums[k], axis=0, keepdims=True)
        cgs[pl.ds(rows, 8), pl.ds(0, size)] = jnp.zeros((8, size), F32)

        @pl.loop(0, rows // chunk)
        def _(n):
            r = pl.multiple_of(n * chunk, chunk)
            wide = cgs[pl.ds(r, chunk + 8), pl.ds(0, size)]
            g1 = pltpu.roll(wide, chunk + 7, 0)[:chunk]
            g2 = pltpu.roll(wide, chunk + 6, 0)[:chunk]
            gst[pl.ds(PAD + r, chunk), cut] = (w2 * wide[:chunk] + w1 * g1 + w0 * g2).astype(BF16)

    def grad_ref(is_gate, at, size):
        ref = gst.at[pl.ds(PAD, rows)] if is_gate else hst
        return columns_of(ref, at, size)

    def grad_copies(g):
        _, _, segments = pieces[g]
        into = getattr(own, f"pg{g}")
        return [
            remote(
                grad_ref(is_gate, at, size), columns_of(into, to, size),
                own.g_ss.at[g, n], own.g_rs.at[g, n], other,
            )
            for n, (is_gate, at, to, size) in enumerate(segments)
        ]

    ready = 0
    for g, (_, _, segments) in enumerate(pieces):
        need = max(at + size for _, at, _, size in segments)
        if need > ready:
            tiles(need - ready, LANES, elementwise, ready)
            ready = need
        for copy in grad_copies(g):
            copy.start()
    if ready < cols:
        tiles(cols - ready, LANES, elementwise, ready)

    def conv_copy(r):
        return remote(csum.at[pl.ds(0, 4)], conv_recv.at[r], own.cs.at[r], own.cr.at[r], me ^ (1 << r))

    def conv_add(r):
        conv_copy(r).wait_send()
        conv_copy(r).wait_recv()
        csum[pl.ds(0, 4), :] += conv_recv[r]

    turns = [*range(1, rounds), 0]
    conv_copy(turns[0]).start()

    part_b(other, bx, other).wait_recv()
    along(part_b, other, b_up, b_down, has_up, has_down)

    def gather(t):
        low, high = i - t - 1, i + t + 1

        @pl.when(low >= 0)
        def _():
            o = 2 * low + j
            part_a(o, a_up, up).wait_recv()
            along(part_a, o, a_up, a_down, has_up, False)

        @pl.when(high < line)
        def _():
            o = 2 * high + j
            part_a(o, a_down, down).wait_recv()
            along(part_a, o, a_up, a_down, False, has_down)

        for flip in range(2):
            jd = j if flip == 0 else 1 - j

            @pl.when(low >= 0)
            def _():
                o = 2 * low + jd
                part_b(o, b_up, up).wait_recv()
                along(part_b, o, b_up, b_down, has_up, False)

            @pl.when(high < line)
            def _():
                o = 2 * high + jd
                part_b(o, b_down, down).wait_recv()
                along(part_b, o, b_up, b_down, False, has_down)

    def left_rows(o):
        return pl.ds(pl.multiple_of(o * shard, shard), shard)

    def term_b(o):
        def one(at, size):
            grad = hst[:, pl.ds(pl.multiple_of(at + split, LANES), size)]
            acc[:, pl.ds(at, size)] = dot_rows(tok_t[left_rows(o), :], grad)

        tiles(wide_b, 256, one)

    def term_a(g, d):
        from_pair = getattr(own, f"pg{g}")
        for is_gate, first, to, count in pieces[g][2]:
            def one(at, size):
                cut = pl.ds(at, size)
                if is_gate:
                    grad = gst[pl.ds(PAD, rows), pl.ds(pl.multiple_of(at - to + first, LANES), size)]
                else:
                    grad = hst[:, pl.ds(pl.multiple_of(at - to + first, LANES), size)]
                total = dot_rows(tok_t[left_rows(2 * d + j), :], grad)
                acc[:, cut] = total + dot_rows(pair_tok[left_rows(d), :], from_pair[:, cut])

            tiles(count, 256, one, to)

    step_rows = 16

    def each_rows(body):
        @pl.loop(0, shard // step_rows)
        def _(n):
            body(pl.ds(pl.multiple_of(n * step_rows, step_rows), step_rows))

    def put(dst, *more):
        span = pl.ds(0, dst.shape[-1])

        def body(cut):
            total = acc[cut, span]
            for ref in more:
                total = total + ref[cut, :].astype(F32)
            dst[cut, span] = total.astype(dst.dtype)

        each_rows(body)

    def unit(w, jd=0):
        if w == 0:
            return own.sb.at[jd], own.sb_ss.at[jd], own.sb_rs.at[jd], lambda d: term_b(2 * d + jd)
        return getattr(own, f"sa{w - 1}"), own.sa_ss.at[w - 1], own.sa_rs.at[w - 1], lambda d: term_a(w - 1, d)

    def level(w, h, jd=0):
        slots, ss, rs, term = unit(w, jd)
        going_up, going_down = i == h, i == line - 1 - h

        @pl.when(going_up | going_down)
        def _():
            @pl.loop(0, line - 1 - h)
            def _(n):
                d = jnp.where(going_up, line - 1 - n, n)
                ahead = jnp.where(going_up, i + 1, i - 1)
                to = jnp.where(going_down & (d == ahead), line, d)
                slot = slots.at[d]
                term(d)
                if h:
                    remote(slot, slot, ss.at[d], rs.at[d]).wait_recv()
                    put(slot, slot)
                else:
                    put(slot)
                remote(slot, slots.at[to], ss.at[d], rs.at[to], 2 * ahead + j).start()

    def arrive(w, jd, finish):
        slots, ss, rs, term = unit(w, jd)
        low, high = slots.at[i], slots.at[line]
        term(i)

        @pl.when(has_down)
        def _():
            remote(low, low, ss.at[i], rs.at[i]).wait_recv()

        @pl.when(has_up)
        def _():
            remote(high, high, ss.at[i], rs.at[line]).wait_recv()

        @pl.when(has_down & has_up)
        def _():
            finish(low, high)

        @pl.when(jnp.logical_not(has_up))
        def _():
            finish(low)

        @pl.when(jnp.logical_not(has_down))
        def _():
            finish(high)

    def share_copy(k, o):
        return remote(ig_send.at[k, o], ig_recv.at[tp, o], own.ig_ss.at[k, o], own.ig_rs.at[tp, o], to_tp=k)

    def share(at, column):
        o = 2 * at + column

        @pl.loop(1, n_tp + 1)
        def _(step):
            k = (tp + step) % n_tp
            start = pl.multiple_of(k * own_tok, own_tok)
            here = pl.ds(start, own_tok)
            part = dot_cols(hst[here, pl.ds(split, wide_b)], wb[o])
            if column is j:
                part = part + dot_cols(gst[pl.ds(PAD + start, own_tok), :], wa[at, :, pl.ds(split, cols)])
                if split:
                    part = part + dot_cols(hst[here, pl.ds(0, split)], wa[at, :, pl.ds(0, split)])
            ig_send[k, o] = part.astype(BF16)

            @pl.when(k != tp)
            def _():
                share_copy(k, o).start()

    def share_far(t):
        for at in (i - t, i + t):
            @pl.when((at >= 0) & (at < line))
            def _():
                share(at, j)
                share(at, 1 - j)

    def pair_share_copy(k, at):
        return remote(own.pi_send.at[k, at], own.pi_recv.at[tp, at], own.pi_ss.at[k, at], own.pi_rs.at[tp, at], to_tp=k)

    def pair_shares():
        @pl.loop(0, line)
        def _(at):
            @pl.loop(0, n_tp)
            def _(n):
                k = 2 * ((tp // 2 + 1 + n // 2) % chips) + (core + n + 1) % 2
                here = pl.ds(pl.multiple_of(k * own_tok, own_tok), own_tok)
                part = None
                for g, (first, size, _) in enumerate(pieces):
                    one = dot_cols(getattr(own, f"pg{g}")[here, :], wa[at, :, pl.ds(first, size)])
                    part = one if part is None else part + one
                own.pi_send[k, at] = part.astype(BF16)

                @pl.when(k != tp)
                def _():
                    pair_share_copy(k, at).start()

    def back(at):
        return remote(own.ret_out.at[at], own.ret_in.at[at], own.ret_ss.at[at], own.ret_rs.at[at], other)

    def pair_shares_back(first, last):
        @pl.loop(first, last)
        def _(at):
            @pl.loop(1, n_tp)
            def _(step):
                pair_share_copy((tp + step) % n_tp, at).wait_send()
                source = (tp + step) % n_tp
                remote(
                    own.pi_send.at[source, at], own.pi_recv.at[source, at],
                    own.pi_ss.at[source, at], own.pi_rs.at[source, at],
                ).wait_recv()

            total = own.pi_send[tp, at].astype(F32)
            for step in range(1, n_tp):
                total = total + own.pi_recv[(tp + step) % n_tp, at].astype(F32)
            own.ret_out[at] = total.astype(BF16)
            back(at).start()

    def finish_piece(g):
        def finish(*refs):
            def body(cut):
                total = acc[cut, pl.ds(0, pieces[g][1])]
                for ref in refs:
                    total = total + ref[cut, :].astype(F32)
                total = total * scale
                for is_gate, at, to, size in pieces[g][2]:
                    (gfin if is_gate else vfin)[cut, pl.ds(at, size)] = total[:, to : to + size]

            each_rows(body)

        arrive(g + 1, 0, finish)

    @pl.loop(0, line)
    def _(n):
        tok_relayed(far(n))

    pair_tokens_out()

    @pl.loop(0, line)
    def _(n):
        tok_landed(far(n))

    waves = len(pieces) + 1
    cross = remote(own.vx_out, own.vx_in, own.xs, own.xr, other)
    returned = 0
    for s in range(waves + line - 2):
        for w in range(waves):
            if s == line and w == waves - 1 and s > max(waves - 1, line - 2):
                pair_shares_back(returned, returned + 1)
                returned += 1
            if w and s == w:
                if w == 1:
                    pair_tokens_in()
                for copy in grad_copies(w - 1):
                    copy.wait_recv()
            if 0 <= s - w < line - 1:
                for jd in range(2 if w == 0 else 1):
                    level(w, s - w, jd)
        if s == 0:
            share(i, j)
            share(i, 1 - j)
        if s < line - 1:
            gather(s)
            share_far(s + 1)
        if s % 2 == 0 and s // 2 < rounds:
            conv_add(turns[s // 2])
            if s // 2 + 1 < rounds:
                conv_copy(turns[s // 2 + 1]).start()
        if s == max(waves - 1, line - 2):
            pair_shares()
        if s == line - 1:
            for mine in (False, True):
                column = j if mine else 1 - j
                finish = (
                    (lambda *refs: put(columns_of(vfin, split, wide_b), *refs))
                    if mine
                    else (lambda *refs: put(own.vx_out, *refs))
                )
                arrive(0, column, finish)
                if not mine:
                    cross.start()
        if s >= line - 1 and s >= waves - 1 and returned < line:
            pair_shares_back(returned, returned + 1)
            returned += 1
        g = s - line
        if 0 <= g < len(pieces) - 1:
            finish_piece(g)

    conv_out[...] = csum[pl.ds(0, 3), :] * scale
    bias_out[...] = (csum[pl.ds(3, 1), :] * scale).reshape(cols)
    pair_shares_back(returned, line)
    for g in range(max(0, waves - 2), len(pieces) - 1):
        finish_piece(g)
    cross.wait_recv()

    def finish_value(cut):
        rest = pl.ds(split, wide_b)
        vfin[cut, rest] = (vfin[cut, rest] + own.vx_in[cut, :].astype(F32)) * scale

    each_rows(finish_value)

    @pl.loop(0, n_fs)
    def _(o):
        @pl.loop(1, n_tp)
        def _(step):
            source = (tp + step) % n_tp
            remote(
                ig_send.at[source, o], ig_recv.at[source, o], own.ig_ss.at[source, o], own.ig_rs.at[source, o]
            ).wait_recv()

    for o in range(n_fs):
        if o % 2 == 0:
            back(o // 2).wait_recv()
        total = ig_send[tp, o].astype(F32)
        for step in range(1, n_tp):
            total = total + ig_recv[(tp + step) % n_tp, o].astype(F32)
        total = total + jnp.where(o % 2 != j, own.ret_in[o // 2].astype(F32), 0.0)
        ig_sum[:, o * shard : (o + 1) * shard] = total.astype(BF16)

    finish_piece(len(pieces) - 1)

    part_b(me, bx, other).wait_send()
    cross.wait_send()
    for g in range(len(pieces)):
        for copy in grad_copies(g):
            copy.wait_send()
    pair_cols(tp, own.pt_relay.at[tp], twin).wait_send()

    @pl.loop(1, chips)
    def _(step):
        source = on_chip(step)
        pair_cols(tp, own.pt_ss.at[source], source).wait_send()
        pair_cols(source, own.pt_relay.at[source], twin).wait_send()

    @pl.loop(0, line)
    def _(d):
        @pl.loop(1, chips)
        def _(step):
            source = on_chip(step)
            tok_copy(d, tp, tok_ss.at[source, d], source).wait_send()
            tok_copy(d, source, tok_relay.at[source, d], twin).wait_send()

        tok_copy(d, tp, tok_relay.at[tp, d], twin).wait_send()
        pair_piece(d).wait_send()
        back(d).wait_send()

        @pl.when(has_up & (d <= i))
        def _():
            part_a(2 * d, a_up, up).wait_send()
            part_b(2 * d, b_up, up).wait_send()
            part_b(2 * d + 1, b_up, up).wait_send()

        @pl.when(has_down & (d >= i))
        def _():
            part_a(2 * d, a_down, down).wait_send()
            part_b(2 * d, b_down, down).wait_send()
            part_b(2 * d + 1, b_down, down).wait_send()

        @pl.when(d != i)
        def _():
            for w in range(waves):
                for jd in range(2 if w == 0 else 1):
                    slots, ss, rs, _ = unit(w, jd)
                    remote(slots.at[d], slots.at[d], ss.at[d], rs.at[d]).wait_send()

    @pl.loop(0, n_fs)
    def _(o):
        @pl.loop(1, n_tp)
        def _(step):
            share_copy((tp + step) % n_tp, o).wait_send()


def scratch_of(line, n_tp, split, pieces, rows, cols, own_tok, width, shard, rounds):
    n_fs, parts, wide_b = 2 * line, len(pieces), cols - split
    dma = pltpu.SemaphoreType.DMA
    widest = max([wide_b] + [size for _, size, _ in pieces])
    table = dict(
        wa=pltpu.VMEM((line, shard, cols + split), BF16),
        wb=pltpu.VMEM((n_fs, shard, wide_b), BF16),
        tok=pltpu.VMEM((own_tok, width), BF16),
        tok_t=pltpu.VMEM((width, rows), BF16),
        pair_tok=pltpu.VMEM((line * shard, rows), BF16),
        gst=pltpu.VMEM((PAD + rows, cols), BF16),
        hst=pltpu.VMEM((rows, cols), BF16),
        vst=pltpu.VMEM((rows, cols), BF16),
        cgs=pltpu.VMEM((rows + 8, LANES), F32),
        acc=pltpu.VMEM((shard, widest), F32),
        sb=pltpu.VMEM((2, line + 1, shard, wide_b), BF16),
        vx_out=pltpu.VMEM((shard, wide_b), BF16),
        vx_in=pltpu.VMEM((shard, wide_b), BF16),
        ig_send=pltpu.VMEM((n_tp, n_fs, own_tok, shard), BF16),
        ig_recv=pltpu.VMEM((n_tp, n_fs, own_tok, shard), BF16),
        pi_send=pltpu.VMEM((n_tp, line, own_tok, shard), BF16),
        pi_recv=pltpu.VMEM((n_tp, line, own_tok, shard), BF16),
        ret_out=pltpu.VMEM((line, own_tok, shard), BF16),
        ret_in=pltpu.VMEM((line, own_tok, shard), BF16),
        conv_recv=pltpu.VMEM((rounds, 4, cols), F32),
        csum=pltpu.VMEM((8, cols), F32),
        load_sem=dma((7,)),
        tok_ss=dma((n_tp, line)), tok_relay=dma((n_tp, line)), tok_rs=dma((n_tp, line)),
        px_ss=dma((line,)), px_rs=dma((line,)),
        pt_ss=dma((n_tp,)), pt_relay=dma((n_tp,)), pt_rs=dma((n_tp,)),
        a_up=dma((line,)), a_down=dma((line,)), ra=dma((line,)),
        b_up=dma((n_fs,)), b_down=dma((n_fs,)), bx=dma((n_fs,)), rb=dma((n_fs,)),
        g_ss=dma((parts, 2)), g_rs=dma((parts, 2)),
        sb_ss=dma((2, line)), sb_rs=dma((2, line + 1)),
        sa_ss=dma((parts, line)), sa_rs=dma((parts, line + 1)),
        xs=dma, xr=dma, ret_ss=dma((line,)), ret_rs=dma((line,)),
        ig_ss=dma((n_tp, n_fs)), ig_rs=dma((n_tp, n_fs)),
        pi_ss=dma((n_tp, line)), pi_rs=dma((n_tp, line)),
        cs=dma((rounds,)), cr=dma((rounds,)),
    )
    for g, (_, size, _) in enumerate(pieces):
        table[f"pg{g}"] = pltpu.VMEM((rows, size), BF16)
        table[f"sa{g}"] = pltpu.VMEM((line + 1, shard, size), BF16)
    return table


def on_device(
    tokens, gate_pre, value_pre, up_gate_w, up_value_w, conv_weight, conv_bias, hidden_grad
):
    n_fs, n_tp = lax.axis_size("fs"), lax.axis_size("tp")
    line = n_fs // 2
    rows, cols = gate_pre.shape
    own_tok, width = tokens.shape
    shard = up_gate_w.shape[0]
    rounds = n_fs.bit_length() - 1
    assert n_fs == 1 << rounds and line >= max(4, rounds) and shard * n_fs == width and n_tp % 2 == 0
    scale = float(rows * n_fs) ** (-0.5)
    split = 0 if cols % LANES else cols * SPLIT // (11 * LANES) * LANES
    pieces = groups_of(cols, split)
    table = scratch_of(line, n_tp, split, pieces, rows, cols, own_tok, width, shard, rounds)
    any_space = pl.BlockSpec(memory_space=pl.ANY)
    vmem = pl.BlockSpec(memory_space=pltpu.VMEM)
    input_grad, gate_out, value_out, conv, bias = pl.pallas_call(
        functools.partial(kernel, line, n_tp, split, pieces, tuple(table), scale),
        out_shape=(
            pltpu.VMEM((own_tok, width), BF16),
            pltpu.VMEM((shard, cols), F32),
            pltpu.VMEM((shard, cols), F32),
            pltpu.VMEM((3, cols), F32),
            pltpu.VMEM((cols,), F32),
        ),
        in_specs=[any_space] * 6 + [vmem] * 2,
        out_specs=(vmem,) * 5,
        scratch_shapes=list(table.values()),
        compiler_params=pltpu.CompilerParams(
            collective_id=0, has_side_effects=True, vmem_limit_bytes=61_000_000
        ),
        name="backward",
    )(
        tokens, gate_pre, value_pre, up_gate_w, up_value_w, hidden_grad,
        conv_weight, conv_bias,
    )
    return (input_grad, gate_out, value_out, conv, bias)


def solution(mesh):
    return jax.shard_map(
        on_device,
        mesh=mesh,
        in_specs=(
            P(("fs", "tp"), None),
            P("fs", "tp"),
            P("fs", "tp"),
            P("fs", "tp"),
            P("fs", "tp"),
            P(None, "tp"),
            P("tp"),
            P("fs", "tp"),
        ),
        out_specs=(P(("fs", "tp"), None), P("fs", "tp"), P("fs", "tp"), P(None, "tp"), P("tp")),
        check_vma=False,
    )
```
